32 devices in a mesh: sp: 4 (over z), fs: 4 (over y, x), tp: 2 (over core).
Axes of the slice: x: 2, y: 2, z: 4, core: 2. Of those that a mesh axis runs over, the one named last changes fastest.
Arguments:
- tokens: bfloat16 [4, 3072, 2048], P('fs', 'sp'), may hold values from -6 to 6
- norm_gain: float32 [2048], replicated, may hold values from 0.1 to 1.9
- w_query: bfloat16 [2048, 512], P('sp', 'tp'), may hold values from -0.125 to 0.125
- w_key: bfloat16 [2048, 512], P('sp', 'tp'), may hold values from -0.125 to 0.125
- w_value: bfloat16 [2048, 1024], P('sp', 'tp'), may hold values from -0.125 to 0.125
- w_conv_value: bfloat16 [2048, 1024], P('sp', 'tp'), may hold values from -0.125 to 0.125
- w_conv_gate: bfloat16 [2048, 1024], P('sp', 'tp'), may hold values from -0.125 to 0.125
- w_decay_low: bfloat16 [2048, 16], replicated, may hold values from -0.125 to 0.125
- w_decay_high: bfloat16 [16, 512], replicated, may hold values from -1.5 to 1.5
- gate_bias: float32 [512], replicated, may hold values from 0.5 to 10
- decay_shift: float32 [4, 3072, 512], P('fs', 'sp', 'tp'), may hold values from -0.6 to 0
- head_gain: float32 [512], replicated, may hold values from 0.1 to 1.9
- conv_taps: float32 [31, 1024], replicated, may hold values from -15 to 15
- channel_gain: float32 [1024], replicated, may hold values from 0.1 to 1.9
- w_out_attn: bfloat16 [1024, 2048], P('tp', 'sp'), may hold values from -0.125 to 0.125
- w_out_conv: bfloat16 [1024, 2048], P('tp', 'sp'), may hold values from -0.125 to 0.125
- init_state: float32 [4, 2, 256, 512], P('fs', 'tp'), may hold values from -332.55374 to 332.55374
Outputs:
- mixed: bfloat16 [4, 3072, 2048], P('fs', ('sp', 'tp'))
The draws below stay inside these ranges and needn't reach their ends.
All inputs are finite; a program needn't handle non-finite values.
Results may differ from the reference program's by a relative error of at most 0.0056.
The reference program's roundings to bfloat16 on the way (of `normed`, `low_rank`, `attn_out`, `glu` and `conv_out`) count: a program that leaves them out, or rounds other values in their place, can miss the bound.
Values may be sent and summed in bfloat16 or wider, within the bound.
A program may use at most 128 MiB of HBM per device.

```python
import math
import jax
import jax.numpy as jnp
from jax import lax

D = 2048
GHEADS = 2
DK = 256
DV = 512
CW = 1024
RANK = 16
KW = 31
BLOCK = 64
T_DEV = 768
SEQS = 4
LENGTH = 3072
GKW = 512
GVW = 1024


def draw_gate_bias(key, part):
    pick_key, slow_key, fast_key = jax.random.split(jax.random.fold_in(key, 11), 3)
    share = 0.5
    chosen = jax.random.uniform(pick_key, (GKW,), jnp.float32) < share
    slow_values = jax.random.uniform(slow_key, (GKW,), jnp.float32, 8.0, 10.0)
    fast_values = jax.random.uniform(fast_key, (GKW,), jnp.float32, 0.5, 1.5)
    return jnp.where(chosen, slow_values, fast_values)


def draw_decay_shift(key, part):
    rate_key, mark_key, depth_key = jax.random.split(jax.random.fold_in(key, 23), 3)
    nblocks = LENGTH // T_DEV
    rates = jnp.exp(jax.random.uniform(rate_key, (SEQS, nblocks, 1, GKW), jnp.float32, math.log(0.2), math.log(1.0))) / LENGTH
    steady = jnp.broadcast_to(rates, (SEQS, nblocks, T_DEV, GKW)).reshape(SEQS, LENGTH, GKW)
    marks = jax.random.uniform(mark_key, (SEQS, LENGTH, 1), jnp.float32) < 3.0 / LENGTH
    depths = jax.random.uniform(depth_key, (SEQS, LENGTH, GKW), jnp.float32, 0.22, 0.5)
    return -steady - jnp.where(marks, depths, 0.0)


def draw_conv_taps(key, part):
    base_key, jitter_key = jax.random.split(jax.random.fold_in(key, 37))
    base = jnp.clip(jax.random.normal(base_key, (KW, CW), jnp.float32), -4.0, 4.0) / math.sqrt(KW)
    channel = jnp.arange(CW, dtype=jnp.float32) / CW
    jitter = jnp.exp(jax.random.uniform(jitter_key, (1, CW), jnp.float32, math.log(0.5), math.log(2.0)))
    return base * jnp.exp(math.log(10.0) * channel) * jitter


def shard_levels(rng, shape, shards, least, top_value):
    def one(dim, shards_of):
        steps = jax.random.uniform(jax.random.fold_in(jax.random.fold_in(rng, 6), dim), (shards_of,), jnp.float32, least / len(shards), top_value / len(shards))
        return jnp.repeat(jnp.exp(steps), shape[dim] // shards_of).reshape((-1,) + (1,) * (len(shape) - dim - 1))

    factor_of = one(*shards[0])
    for cut in shards[1:]:
        factor_of = factor_of * one(*cut)
    return factor_of


def noise(own_key, extent, spread, most, pieces=(), kind=jnp.bfloat16):
    drawn = spread * jax.random.normal(own_key, extent, jnp.float32)
    if pieces:
        drawn = drawn * shard_levels(own_key, extent, pieces, -0.22, 0.18)
    return jnp.clip(drawn, -most, most).astype(kind)


def setup_inputs(seed: int = 0) -> dict:
    keys = jax.random.split(jax.random.key(seed), 18)
    return {
        "tokens": noise(keys[0], (SEQS, LENGTH, D), 1.0, 6.0, ((0, 4), (1, 4))),
        "norm_gain": jnp.clip(1.0 + 0.18 * jax.random.normal(keys[1], (D,), jnp.float32), 0.1, 1.9),
        "w_query": noise(keys[2], (D, GKW), D ** -0.5, 0.125, ((0, 4), (1, 2))),
        "w_key": noise(keys[3], (D, GKW), D ** -0.5, 0.125, ((0, 4), (1, 2))),
        "w_value": noise(keys[4], (D, GVW), D ** -0.5, 0.125, ((0, 4), (1, 2))),
        "w_conv_value": noise(keys[5], (D, CW), D ** -0.5, 0.125, ((0, 4), (1, 2))),
        "w_conv_gate": noise(keys[6], (D, CW), D ** -0.5, 0.125, ((0, 4), (1, 2))),
        "w_decay_low": noise(keys[7], (D, RANK), D ** -0.5, 0.125),
        "w_decay_high": noise(keys[8], (RANK, GKW), RANK ** -0.5, 1.5),
        "gate_bias": draw_gate_bias(jax.random.fold_in(keys[17], 71), 0),
        "decay_shift": draw_decay_shift(jax.random.fold_in(keys[17], 71), 0),
        "head_gain": jnp.clip(1.0 + 0.18 * jax.random.normal(keys[11], (DV,), jnp.float32), 0.1, 1.9),
        "conv_taps": draw_conv_taps(jax.random.fold_in(keys[17], 71), 0),
        "channel_gain": jnp.clip(1.0 + 0.18 * jax.random.normal(keys[13], (CW,), jnp.float32), 0.1, 1.9),
        "w_out_attn": noise(keys[14], (GVW, D), (GVW + CW) ** -0.5, 0.125, ((0, 2), (1, 4))),
        "w_out_conv": noise(keys[15], (CW, D), (GVW + CW) ** -0.5, 0.125, ((0, 2), (1, 4))),
        "init_state": noise(keys[16], (SEQS, GHEADS, DK, DV), (LENGTH ** 0.5), 332.55374, ((0, 4), (1, 2)), jnp.float32),
    }


RMS_EPS = 1e-06
LN_EPS = 1e-05
GATE_NORMALIZER = 16.0
UPPER_PRECISION = lax.Precision.HIGHEST

def rounded(array):
    return lax.optimization_barrier(array.astype(jnp.bfloat16)).astype(jnp.float32)

def one_sequence(token_rows, shift_log, start_state, norm_gain, w_query, w_key, w_value, w_conv_value, w_conv_gate, w_decay_low, w_decay_high, gate_bias, head_gain, conv_taps, channel_gain, w_out_attn, w_out_conv):
    rows_float = token_rows.astype(jnp.float32)
    normed = (rows_float * lax.rsqrt(lax.optimization_barrier(jnp.mean(rows_float * rows_float, axis=1, keepdims=True)) + RMS_EPS) * norm_gain).astype(jnp.bfloat16)
    queries = rounded(jnp.dot(normed, w_query, preferred_element_type=jnp.float32))
    keys_proj = rounded(jnp.dot(normed, w_key, preferred_element_type=jnp.float32))
    values_proj = rounded(jnp.dot(normed, w_value, preferred_element_type=jnp.float32))
    low_rank = jnp.dot(normed, w_decay_low, preferred_element_type=jnp.float32).astype(jnp.bfloat16)
    log_decay = jax.nn.log_sigmoid(jnp.dot(low_rank, w_decay_high, preferred_element_type=jnp.float32) + gate_bias) / GATE_NORMALIZER + shift_log
    nblocks = LENGTH // BLOCK

    def blocks_of(array, width):
        return array.reshape(nblocks, BLOCK, GHEADS, width).transpose(0, 2, 1, 3)
    query_blocks = blocks_of(queries, DK) * DK ** (-0.5)
    key_blocks = blocks_of(keys_proj, DK)
    value_blocks = blocks_of(values_proj, DV)
    decay_blocks = blocks_of(log_decay, DK)
    lower = jnp.tril(jnp.ones((BLOCK, BLOCK), jnp.float32))

    def step(recurrent_state, inputs):
        query_now, current_key, current_value, decay_now = inputs
        running_total = jnp.cumsum(decay_now, axis=1)
        final_entry = running_total[:, -1:, :]
        scaled_query = query_now * jnp.exp(running_total)
        key_scaled = current_key * jnp.exp(-running_total)
        attention_scores = jnp.einsum('hik,hjk->hij', scaled_query, key_scaled, precision=UPPER_PRECISION) * lower
        output_rows = jnp.einsum('daw,dwk->dak', attention_scores, current_value, precision=UPPER_PRECISION) + jnp.einsum('fmb,fbw->fmw', scaled_query, recurrent_state, precision=UPPER_PRECISION)
        state_update = jnp.einsum('adp,adi->api', current_key * jnp.exp(final_entry - running_total), current_value, precision=UPPER_PRECISION)
        recurrent_state = jnp.exp(final_entry[:, 0, :])[:, :, None] * recurrent_state + state_update
        return (recurrent_state, output_rows)
    final_state, attended = lax.scan(step, start_state, (query_blocks, key_blocks, value_blocks, decay_blocks))
    mean_square = lax.optimization_barrier(jnp.mean(attended * attended, axis=3, keepdims=True))
    attn_out = (attended * lax.rsqrt(mean_square + RMS_EPS) * head_gain).astype(jnp.bfloat16)
    attn_out = attn_out.transpose(0, 2, 1, 3).reshape(LENGTH, GVW)
    conv_value = jnp.dot(normed, w_conv_value, preferred_element_type=jnp.float32)
    conv_gate = jnp.dot(normed, w_conv_gate, preferred_element_type=jnp.float32)
    glu = rounded(conv_value * jax.nn.sigmoid(conv_gate))
    padded = jnp.pad(glu, ((KW - 1, 0), (0, 0)))
    filtered = jnp.zeros((LENGTH, CW), jnp.float32)
    for tap_index in range(KW):
        filtered = filtered + conv_taps[tap_index] * padded[tap_index:tap_index + LENGTH]
    mean = lax.optimization_barrier(jnp.mean(filtered, axis=1, keepdims=True))
    centered = filtered - mean
    variance = lax.optimization_barrier(jnp.mean(centered * centered, axis=1, keepdims=True))
    conv_out = jax.nn.silu(centered * lax.rsqrt(variance + LN_EPS) * channel_gain).astype(jnp.bfloat16)
    joined = jnp.concatenate([attn_out, conv_out], axis=1)
    weights = jnp.concatenate([w_out_attn, w_out_conv], axis=0)
    return jnp.dot(joined, weights, preferred_element_type=jnp.float32).astype(jnp.bfloat16)

def reference(tokens, norm_gain, w_query, w_key, w_value, w_conv_value, w_conv_gate, w_decay_low, w_decay_high, gate_bias, decay_shift, head_gain, conv_taps, channel_gain, w_out_attn, w_out_conv, init_state):

    def per_sequence(items):
        return one_sequence(items[0], items[1], items[2], norm_gain, w_query, w_key, w_value, w_conv_value, w_conv_gate, w_decay_low, w_decay_high, gate_bias, head_gain, conv_taps, channel_gain, w_out_attn, w_out_conv)
    return lax.map(per_sequence, (tokens, decay_shift, init_state))
```

```python
import jax
import jax.numpy as jnp
from jax import lax
from jax.sharding import PartitionSpec as P

DK = 256
DV = 512
CW = 1024
KW = 31
BLOCK = 64


RMS_EPS = 1e-06
LN_EPS = 1e-05
GATE_NORMALIZER = 16.0
UPPER_PRECISION = lax.Precision.HIGHEST


def entering(array, axis, combine, identity):
    size, place = (lax.axis_size(axis), lax.axis_index(axis))
    everything = jax.tree.map(lambda part: lax.all_gather(part, axis), array)
    start = jax.tree.map(
        lambda part, zero: jnp.broadcast_to(jnp.asarray(zero, part.dtype), part.shape),
        array,
        identity,
    )

    def turn(k, before):
        reached = k < place
        new = combine(before, jax.tree.map(lambda part: part[k], everything))
        return jax.tree.map(lambda a, b: jnp.where(reached, a, b), new, before)

    return lax.fori_loop(0, size, turn, start)


def shifted(value, axis, steps):
    count = lax.axis_size(axis)
    initial, last = (max(0, -steps), min(count, count - steps))
    return lax.ppermute(value, axis, [(source, source + steps) for source in range(initial, last)])


def rounded(array):
    return lax.optimization_barrier(array.astype(jnp.bfloat16)).astype(jnp.float32)


def spread_gather(*weights):
    turns = lax.axis_size("fs")
    rows = weights[0].shape[0] // turns
    start = lax.axis_index("fs") * rows
    piece = jnp.concatenate(
        [lax.dynamic_slice_in_dim(weight, start, rows, 0) for weight in weights], axis=1
    )
    return lax.all_gather(piece, ("sp", "fs"), axis=0, tiled=True)


def chain_combine(earlier, later):
    return (earlier[0] * later[0], later[0][..., None] * earlier[1] + later[1])


def on_device(
    tokens,
    norm_gain,
    w_query,
    w_key,
    w_value,
    w_conv_value,
    w_conv_gate,
    w_decay_low,
    w_decay_high,
    gate_bias,
    decay_shift,
    head_gain,
    conv_taps,
    channel_gain,
    w_out_attn,
    w_out_conv,
    init_state,
):
    token_rows = tokens[0].astype(jnp.float32)
    length_here = token_rows.shape[0]
    normed = (
        token_rows
        * lax.rsqrt(jnp.mean(token_rows * token_rows, axis=1, keepdims=True) + RMS_EPS)
        * norm_gain
    ).astype(jnp.bfloat16)
    position = lax.axis_index("tp")
    key_cols = w_query.shape[1]
    value_cols = w_value.shape[1]
    conv_cols = w_conv_value.shape[1]
    heads_here = key_cols // DK
    qkv_weight = spread_gather(w_query, w_key, w_value)
    conv_weight = spread_gather(w_conv_value, w_conv_gate)
    out_weight = spread_gather(w_out_attn, w_out_conv)
    qkv = jnp.dot(normed, qkv_weight, preferred_element_type=jnp.float32)
    queries = qkv[:, :key_cols]
    keys_proj = qkv[:, key_cols : 2 * key_cols]
    values_proj = qkv[:, 2 * key_cols :]
    both = jnp.dot(normed, conv_weight, preferred_element_type=jnp.float32)
    conv_value = both[:, :conv_cols]
    conv_gate = both[:, conv_cols:]
    low_rank = jnp.dot(normed, w_decay_low, preferred_element_type=jnp.float32).astype(jnp.bfloat16)
    high_cols = lax.dynamic_slice_in_dim(w_decay_high, position * key_cols, key_cols, 1)
    bias_here = lax.dynamic_slice_in_dim(gate_bias, position * key_cols, key_cols, 0)
    log_decay = (
        jax.nn.log_sigmoid(
            jnp.dot(low_rank, high_cols, preferred_element_type=jnp.float32) + bias_here
        )
        / GATE_NORMALIZER
        + decay_shift[0]
    )
    nblocks = length_here // BLOCK

    def blocks_of(array, width):
        return array.reshape(nblocks, BLOCK, heads_here, width).transpose(2, 0, 1, 3)

    query_blocks = blocks_of(rounded(queries), DK) * DK ** (-0.5)
    key_blocks = blocks_of(rounded(keys_proj), DK)
    value_blocks = blocks_of(rounded(values_proj), DV)
    decay_blocks = blocks_of(log_decay, DK)
    running_total = jnp.cumsum(decay_blocks, axis=2)
    final_entry = running_total[:, :, -1:, :]
    scaled_query = query_blocks * jnp.exp(running_total)
    key_scaled = key_blocks * jnp.exp(-running_total)
    lower = jnp.tril(jnp.ones((BLOCK, BLOCK), jnp.float32))
    attention_scores = (
        jnp.einsum("hnik,hnjk->hnij", scaled_query, key_scaled, precision=UPPER_PRECISION) * lower
    )
    inner = jnp.einsum("hnij,hnjv->hniv", attention_scores, value_blocks, precision=UPPER_PRECISION)
    updates = jnp.einsum(
        "hnjk,hnjv->hnkv",
        key_blocks * jnp.exp(final_entry - running_total),
        value_blocks,
        precision=UPPER_PRECISION,
    )
    block_decay = jnp.exp(final_entry[:, :, 0, :])

    def carry_step(recurrent_state, items):
        decay_now, update_now = items
        return (decay_now[..., None] * recurrent_state + update_now, recurrent_state)

    local_end, before = lax.scan(
        carry_step,
        jnp.zeros((heads_here, DK, DV), jnp.float32),
        (block_decay.transpose(1, 0, 2), updates.transpose(1, 0, 2, 3)),
    )
    inner = inner + jnp.einsum("hnik,nhkv->hniv", scaled_query, before, precision=UPPER_PRECISION)
    start_positions = jnp.cumsum(final_entry, axis=1) - final_entry
    device_decay = jnp.exp(jnp.sum(final_entry[:, :, 0, :], axis=1))
    decay_before, state_before = entering(
        (device_decay, local_end),
        "sp",
        chain_combine,
        (jnp.ones_like(device_decay), jnp.zeros_like(local_end)),
    )
    incoming_carry = state_before + decay_before[..., None] * init_state[0]
    attended = inner + jnp.einsum(
        "stcl,slu->stcu",
        scaled_query * jnp.exp(start_positions),
        incoming_carry,
        precision=UPPER_PRECISION,
    )
    mean_square = jnp.mean(attended * attended, axis=3, keepdims=True)
    attn_out = (attended * lax.rsqrt(mean_square + RMS_EPS) * head_gain).astype(jnp.bfloat16)
    attn_out = attn_out.transpose(1, 2, 0, 3).reshape(length_here, value_cols)
    glu = (conv_value * jax.nn.sigmoid(conv_gate)).astype(jnp.bfloat16)
    rim = shifted(glu[length_here - (KW - 1) :], "sp", 1)
    padded = jnp.concatenate([rim, glu], axis=0).astype(jnp.float32)
    taps_here = lax.dynamic_slice_in_dim(conv_taps, position * conv_cols, conv_cols, 1)
    filtered = jnp.zeros((length_here, conv_cols), jnp.float32)
    for tap_index in range(KW):
        filtered = filtered + taps_here[tap_index] * padded[tap_index : tap_index + length_here]
    first_sum, square_sum = lax.psum(
        (
            jnp.sum(filtered, axis=1, keepdims=True),
            jnp.sum(filtered * filtered, axis=1, keepdims=True),
        ),
        "tp",
    )
    mean = first_sum / CW
    centered = filtered - mean
    variance = square_sum / CW - mean * mean
    gain_here = lax.dynamic_slice_in_dim(channel_gain, position * conv_cols, conv_cols, 0)
    conv_out = jax.nn.silu(centered * lax.rsqrt(variance + LN_EPS) * gain_here).astype(jnp.bfloat16)
    parts = lax.axis_size("sp")
    width = w_out_attn.shape[1]
    out_weight = out_weight.reshape(parts, value_cols, 2 * width)
    columns = jnp.concatenate(
        [
            jnp.dot(attn_out, out_weight[z, :, :width], preferred_element_type=jnp.float32)
            + jnp.dot(conv_out, out_weight[z, :, width:], preferred_element_type=jnp.float32)
            for z in range(parts)
        ],
        axis=1,
    )
    half = length_here // 2
    kept = lax.dynamic_slice_in_dim(columns, position * half, half, 0)
    given = lax.dynamic_slice_in_dim(columns, (1 - position) * half, half, 0).astype(jnp.bfloat16)
    mixed = kept + lax.ppermute(given, "tp", [(0, 1), (1, 0)]).astype(jnp.float32)
    return mixed.astype(jnp.bfloat16)[None]


def solution(mesh):
    in_specs = (
        P("fs", "sp", None),
        P(),
        P("sp", "tp"),
        P("sp", "tp"),
        P("sp", "tp"),
        P("sp", "tp"),
        P("sp", "tp"),
        P(),
        P(),
        P(),
        P("fs", "sp", "tp"),
        P(),
        P(),
        P(),
        P("tp", "sp"),
        P("tp", "sp"),
        P("fs", "tp", None, None),
    )
    out_specs = P("fs", ("sp", "tp"), None)
    return jax.shard_map(
        on_device, mesh=mesh, in_specs=in_specs, out_specs=out_specs, check_vma=False
    )
```

```python
import functools

import jax
import jax.numpy as jnp
from jax import lax
from jax.experimental import pallas as pl
from jax.experimental.pallas import tpu as pltpu
from jax.sharding import PartitionSpec as P

DK = 256
DV = 512
CW = 1024
KW = 31
BLOCK = 64


RMS_EPS = 1e-06
LN_EPS = 1e-05
GATE_NORMALIZER = 16.0
F32 = jnp.float32
BF16 = jnp.bfloat16


def cost(flops, nbytes):
    return pl.CostEstimate(flops=flops, bytes_accessed=nbytes, transcendentals=0)


def shifted(value, axis, steps):
    count = lax.axis_size(axis)
    initial, last = (max(0, -steps), min(count, count - steps))
    return lax.ppermute(value, axis, [(source, source + steps) for source in range(initial, last)])


def turned(value, steps):
    count = lax.axis_size("sp")
    return lax.ppermute(value, "sp", [(i, (i + steps) % count) for i in range(count)])


def swapped(value, mask):
    return lax.ppermute(value, "fs", [(i, i ^ mask) for i in range(lax.axis_size("fs"))])


def spread(own, after, turn):
    rows = own.shape[0] // lax.axis_size("fs")
    piece = lax.dynamic_slice_in_dim(own, lax.axis_index("fs") * rows, rows, 0)
    if after is not None:
        piece, _ = lax.optimization_barrier((piece, after))
    pieces = []
    for s in range(1, lax.axis_size("sp")):
        mine = turned(piece, s)
        over_x = swapped(mine, 1)
        over_y = swapped(mine, 2)
        if (s + turn) % 2:
            diagonal = swapped(over_y, 1)
        else:
            diagonal = swapped(over_x, 2)
        pieces += [mine, over_x, over_y, diagonal]
    return pieces


def gathered(own):
    rows = own.shape[0] // lax.axis_size("fs")
    piece = lax.dynamic_slice_in_dim(own, lax.axis_index("fs") * rows, rows, 0)
    return lax.all_gather(piece, ("sp", "fs"), axis=0, tiled=True)


def norm_kernel(slots, x_ref, gain_ref, low_ref, high_ref, bias_ref, shift_ref, n_ref, d_ref, *, count):
    x = x_ref[...].astype(F32)
    scale = lax.rsqrt(jnp.mean(x * x, axis=1, keepdims=True) + RMS_EPS)
    normed = (x * scale * gain_ref[...]).astype(BF16)
    width = normed.shape[1] // count
    for i in range(count):
        at = pl.multiple_of(slots[i] * width, width)
        n_ref[:, pl.ds(at, width)] = normed[:, i * width : (i + 1) * width]
    low = jnp.dot(normed, low_ref[...], preferred_element_type=F32).astype(BF16)
    z = jnp.dot(low, high_ref[...], preferred_element_type=F32) + bias_ref[...]
    log_sig = jnp.minimum(z, 0.0) - jnp.log1p(jnp.exp(-jnp.abs(z)))
    d_ref[...] = log_sig / GATE_NORMALIZER + shift_ref[...]


def norm_and_decay(tokens, slots, gain, low, high, bias, shift):
    rows, width = tokens.shape
    tile = rows // 6
    keys = high.shape[1]
    whole = lambda *shape: pl.BlockSpec(shape, lambda i, s: (0, 0))
    tiled = lambda cols: pl.BlockSpec((tile, cols), lambda i, s: (i, 0))
    return pl.pallas_call(
        functools.partial(norm_kernel, count=slots.shape[0]),
        grid_spec=pltpu.PrefetchScalarGridSpec(
            num_scalar_prefetch=1,
            grid=(rows // tile,),
            in_specs=[
                tiled(width),
                whole(1, width),
                whole(*low.shape),
                whole(*high.shape),
                whole(1, keys),
                tiled(keys),
            ],
            out_specs=[tiled(width), tiled(keys)],
        ),
        out_shape=[
            jax.ShapeDtypeStruct((rows, width), BF16),
            jax.ShapeDtypeStruct((rows, keys), F32),
        ],
        cost_estimate=cost(rows * width * 64, rows * width * 4),
        name="norm",
    )(slots, tokens, gain[None], low, high, bias[None], shift)


def project_kernel(x_ref, *refs, gated):
    *pieces, out_ref, weight = refs

    @pl.when(pl.program_id(0) == 0)
    def _():
        at = 0
        for piece in pieces:
            weight[at : at + piece.shape[0], :] = piece[...]
            at += piece.shape[0]

    product = jnp.dot(x_ref[...], weight[...], preferred_element_type=F32)
    if gated:
        half = product.shape[1] // 2
        product = product[:, :half] * jax.nn.sigmoid(product[:, half:])
    out_ref[...] = product.astype(out_ref.dtype)


def project(normed, pieces, gated):
    rows, depth = normed.shape
    cols = pieces[0].shape[1]
    tile = rows // 3
    out_cols = cols // 2 if gated else cols
    return pl.pallas_call(
        functools.partial(project_kernel, gated=gated),
        grid=(rows // tile,),
        in_specs=[pl.BlockSpec((tile, depth), lambda i: (i, 0))]
        + [pl.BlockSpec(piece.shape, lambda i: (0, 0)) for piece in pieces],
        out_specs=pl.BlockSpec((tile, out_cols), lambda i: (i, 0)),
        out_shape=jax.ShapeDtypeStruct((rows, out_cols), BF16),
        scratch_shapes=[pltpu.VMEM((depth, cols), BF16)],
        cost_estimate=cost(2 * rows * depth * cols, 2 * depth * (rows + cols)),
        name="project_gated" if gated else "project",
    )(normed, *pieces)


def dot_t(a, b):
    return lax.dot_general(a, b, (((1,), (1,)), ((), ())), preferred_element_type=F32)


def dot_rows(a, b):
    return lax.dot_general(a, b, (((0,), (0,)), ((), ())), preferred_element_type=F32)


def block_kernel(q_ref, k_ref, v_ref, d_ref, inner_ref, reach_ref, state_ref, total_ref, state, start):
    step = pl.program_id(0)

    @pl.when(step == 0)
    def _():
        state[...] = jnp.zeros_like(state)
        start[...] = jnp.zeros_like(start)

    size = d_ref.shape[0]
    row = lax.broadcasted_iota(jnp.int32, (size, size), 0)
    col = lax.broadcasted_iota(jnp.int32, (size, size), 1)
    lower = (row >= col).astype(F32)
    running = jnp.dot(
        lower, d_ref[...], precision=lax.Precision.HIGHEST, preferred_element_type=F32
    )
    final = running[size - 1 : size, :]
    before = start[0:1, :]
    q = q_ref[...].astype(F32) * DK ** (-0.5)
    k = k_ref[...].astype(F32)
    v = v_ref[...]
    scaled = q * jnp.exp(running)
    reach_ref[...] = (scaled * jnp.exp(before)).astype(BF16)
    scaled = scaled.astype(BF16)
    scores = dot_t(scaled, (k * jnp.exp(-running)).astype(BF16))
    scores = jnp.where(row >= col, scores, 0.0).astype(BF16)
    now = state[...]
    inner_ref[...] = jnp.dot(scores, v, preferred_element_type=F32) + dot_t(scaled, now.astype(BF16))
    later = jnp.exp(final) * now + dot_rows(v, (k * jnp.exp(final - running)).astype(BF16))
    state[...] = later
    start[0:1, :] = before + final

    @pl.when(step == pl.num_programs(0) - 1)
    def _():
        state_ref[...] = later.astype(BF16)
        total_ref[...] = jnp.exp(before + final)


def blocks(qkv, log_decay):
    rows = qkv.shape[0]
    part = lambda width, at: pl.BlockSpec((BLOCK, width), lambda i: (i, at))
    fixed = lambda *shape: pl.BlockSpec(shape, lambda i: (0, 0))
    return pl.pallas_call(
        block_kernel,
        grid=(rows // BLOCK,),
        in_specs=[part(DK, 0), part(DK, 1), part(DV, 1), part(DK, 0)],
        out_specs=[part(DV, 0), part(DK, 0), fixed(DV, DK), fixed(1, DK)],
        out_shape=[
            jax.ShapeDtypeStruct((rows, DV), F32),
            jax.ShapeDtypeStruct((rows, DK), BF16),
            jax.ShapeDtypeStruct((DV, DK), BF16),
            jax.ShapeDtypeStruct((1, DK), F32),
        ],
        scratch_shapes=[pltpu.VMEM((DV, DK), F32), pltpu.VMEM((8, DK), F32)],
        cost_estimate=cost(rows * DK * DV * 10, rows * 8192),
        name="blocks",
    )(qkv, qkv, qkv, log_decay)


def finish_kernel(inner_ref, reach_ref, state_ref, gain_ref, out_ref):
    attended = inner_ref[...] + dot_t(reach_ref[...], state_ref[...])
    mean_square = jnp.mean(attended * attended, axis=1, keepdims=True)
    out_ref[...] = (attended * lax.rsqrt(mean_square + RMS_EPS) * gain_ref[...]).astype(BF16)


def finish(inner, reach, state, gain):
    rows = inner.shape[0]
    tile = rows // 3
    tiled = lambda cols: pl.BlockSpec((tile, cols), lambda i: (i, 0))
    return pl.pallas_call(
        finish_kernel,
        grid=(rows // tile,),
        in_specs=[
            tiled(DV),
            tiled(DK),
            pl.BlockSpec((DV, DK), lambda i: (0, 0)),
            pl.BlockSpec((1, DV), lambda i: (0, 0)),
        ],
        out_specs=tiled(DV),
        out_shape=jax.ShapeDtypeStruct((rows, DV), BF16),
        cost_estimate=cost(rows * DK * DV * 2, rows * 4096),
        name="finish",
    )(inner, reach, state, gain[None])


def out_kernel(where, a_ref, c_ref, own_ref, *refs):
    *pieces, out_ref, weight = refs
    parts = len(pieces) // 4 + 1
    depth, cols = own_ref.shape
    rows = pieces[0].shape[0]

    @pl.when(pl.program_id(0) == 0)
    def _():
        at = pl.multiple_of(where[1] * cols, cols)
        weight[:, pl.ds(at, cols)] = own_ref[...]
        for s in range(1, parts):
            at = pl.multiple_of(lax.rem(where[1] - s + parts, parts) * cols, cols)
            for d in range(4):
                to = pl.multiple_of((where[2] ^ d) * rows, rows)
                weight[pl.ds(to, rows), pl.ds(at, cols)] = pieces[(s - 1) * 4 + d][...]

    half = depth // 2
    out_ref[...] = (
        jnp.dot(a_ref[...], weight[:half, :], preferred_element_type=F32)
        + jnp.dot(c_ref[...], weight[half:, :], preferred_element_type=F32)
    ).astype(out_ref.dtype)


def out_rows(where, attn, conv, own, pieces, dtype):
    rows, depth = attn.shape
    cols = own.shape[1] * lax.axis_size("sp")
    tile = rows // 6
    rowed = pl.BlockSpec((tile, depth), lambda i, w: (w[0] * 3 + i, 0))
    return pl.pallas_call(
        out_kernel,
        grid_spec=pltpu.PrefetchScalarGridSpec(
            num_scalar_prefetch=1,
            grid=(3,),
            in_specs=[rowed, rowed]
            + [pl.BlockSpec(piece.shape, lambda i, w: (0, 0)) for piece in (own, *pieces)],
            out_specs=pl.BlockSpec((tile, cols), lambda i, w: (i, 0)),
            scratch_shapes=[pltpu.VMEM((own.shape[0], cols), BF16)],
        ),
        out_shape=jax.ShapeDtypeStruct((rows // 2, cols), dtype),
        cost_estimate=cost(2 * rows * depth * cols, 4 * depth * cols),
        name="out_rows",
    )(where, attn, conv, own, *pieces)


def on_device(
    tokens,
    norm_gain,
    w_query,
    w_key,
    w_value,
    w_conv_value,
    w_conv_gate,
    w_decay_low,
    w_decay_high,
    gate_bias,
    decay_shift,
    head_gain,
    conv_taps,
    channel_gain,
    w_out_attn,
    w_out_conv,
    init_state,
):
    parts, turns = lax.axis_size("sp"), lax.axis_size("fs")
    place, column = lax.axis_index("sp"), lax.axis_index("fs")
    position = lax.axis_index("tp")
    direct = parts == 4 and turns == 4
    length_here = tokens.shape[1]
    key_cols = w_query.shape[1]
    conv_cols = w_conv_value.shape[1]
    own_qkv = jnp.concatenate([w_query, w_key, w_value], axis=1)
    own_conv = jnp.concatenate([w_conv_value, w_conv_gate], axis=1)
    own_out = jnp.concatenate([w_out_attn, w_out_conv], axis=0)
    if direct:
        index = jnp.arange(parts * turns, dtype=jnp.int32)
        shift = (place - index // turns + parts) % parts
        slots = jnp.where(
            shift == 0, index % turns, turns * shift + ((index % turns) ^ column)
        ).astype(jnp.int32)
        got_qkv = spread(own_qkv, None, 0)
        got_conv = spread(own_conv, got_qkv[8], 1)
        got_out = spread(own_out, got_conv[8], 0)
        all_qkv, all_conv = [own_qkv, *got_qkv], [own_conv, *got_conv]
    else:
        slots = jnp.zeros((1,), jnp.int32)
        all_qkv, all_conv = [gathered(own_qkv)], [gathered(own_conv)]
        out_weight = lax.all_gather(own_out, "sp", axis=1, tiled=True)
    high_cols = lax.dynamic_slice_in_dim(w_decay_high, position * key_cols, key_cols, 1)
    bias_here = lax.dynamic_slice_in_dim(gate_bias, position * key_cols, key_cols, 0)
    normed, log_decay = norm_and_decay(
        tokens[0], slots, norm_gain, w_decay_low, high_cols, bias_here, decay_shift[0]
    )
    qkv = project(normed, all_qkv, False)
    inner, reach, state, total = blocks(qkv, log_decay)
    total_high = total.astype(BF16)
    total_low = (total - total_high.astype(F32)).astype(BF16)
    packed = jnp.concatenate([state, jnp.pad(total_high, ((0, 7), (0, 0))), jnp.pad(total_low, ((0, 7), (0, 0)))], axis=0)
    carried = jnp.zeros((DV, DK), F32)
    decay = jnp.ones((1, DK), F32)
    for s in range(1, parts):
        other = shifted(packed, "sp", s)
        carried = carried + decay * other[:DV].astype(F32)
        gone = other[DV : DV + 1].astype(F32) + other[DV + 8 : DV + 9].astype(F32)
        decay = decay * jnp.where(place >= s, gone, 1.0)
    incoming = (carried + decay * init_state[0, 0].T).astype(BF16)
    attn_out = finish(inner, reach, incoming, head_gain)

    glu = project(normed, all_conv, True)
    rim = shifted(glu[length_here - (KW - 1) :], "sp", 1)
    padded = jnp.concatenate([rim, glu], axis=0).astype(F32)
    taps_here = lax.dynamic_slice_in_dim(conv_taps, position * conv_cols, conv_cols, 1)
    filtered = jnp.zeros((length_here, conv_cols), F32)
    for tap_index in range(KW):
        filtered = filtered + taps_here[tap_index] * padded[tap_index : tap_index + length_here]
    first_sum, square_sum = lax.psum(
        (
            jnp.sum(filtered, axis=1, keepdims=True),
            jnp.sum(filtered * filtered, axis=1, keepdims=True),
        ),
        "tp",
    )
    mean = first_sum / CW
    centered = filtered - mean
    variance = square_sum / CW - mean * mean
    gain_here = lax.dynamic_slice_in_dim(channel_gain, position * conv_cols, conv_cols, 0)
    conv_out = jax.nn.silu(centered * lax.rsqrt(variance + LN_EPS) * gain_here).astype(BF16)

    if direct:
        at = lambda half: jnp.stack([half, place, column]).astype(jnp.int32)
        given = out_rows(at(1 - position), attn_out, conv_out, own_out, got_out, BF16)
        taken = lax.ppermute(given, "tp", [(0, 1), (1, 0)])
        kept = out_rows(at(position), attn_out, conv_out, own_out, got_out, F32)
    else:
        both = jnp.concatenate([attn_out, conv_out], axis=1)
        columns = jnp.dot(both, out_weight, preferred_element_type=F32)
        half = length_here // 2
        kept = lax.dynamic_slice_in_dim(columns, position * half, half, 0)
        given = lax.dynamic_slice_in_dim(columns, (1 - position) * half, half, 0).astype(BF16)
        taken = lax.ppermute(given, "tp", [(0, 1), (1, 0)])
    return (kept + taken.astype(F32)).astype(BF16)[None]


def solution(mesh):
    in_specs = (
        P("fs", "sp", None),
        P(),
        P("sp", "tp"),
        P("sp", "tp"),
        P("sp", "tp"),
        P("sp", "tp"),
        P("sp", "tp"),
        P(),
        P(),
        P(),
        P("fs", "sp", "tp"),
        P(),
        P(),
        P(),
        P("tp", "sp"),
        P("tp", "sp"),
        P("fs", "tp", None, None),
    )
    out_specs = P("fs", ("sp", "tp"), None)
    return jax.shard_map(
        on_device, mesh=mesh, in_specs=in_specs, out_specs=out_specs, check_vma=False
    )
```

```python
import functools

import jax
import jax.numpy as jnp
from jax import lax
from jax.experimental import pallas as pl
from jax.experimental.pallas import tpu as pltpu
from jax.sharding import PartitionSpec as P

DK = 256
DV = 512
CW = 1024
KW = 31
BLOCK = 64


RMS_EPS = 1e-06
LN_EPS = 1e-05
GATE_NORMALIZER = 16.0
F32 = jnp.float32
BF16 = jnp.bfloat16


def cost(flops, nbytes):
    return pl.CostEstimate(flops=flops, bytes_accessed=nbytes, transcendentals=0)


def shifted(value, axis, steps):
    count = lax.axis_size(axis)
    initial, last = (max(0, -steps), min(count, count - steps))
    return lax.ppermute(value, axis, [(source, source + steps) for source in range(initial, last)])


def swapped(value, mask):
    return lax.ppermute(value, "fs", [(i, i ^ mask) for i in range(lax.axis_size("fs"))])


def gathered(own):
    rows = own.shape[0] // lax.axis_size("fs")
    piece = lax.dynamic_slice_in_dim(own, lax.axis_index("fs") * rows, rows, 0)
    return lax.all_gather(piece, ("sp", "fs"), axis=0, tiled=True)


def norm_kernel(x_ref, gain_ref, low_ref, high_ref, bias_ref, shift_ref, n_ref, d_ref):
    x = x_ref[...].astype(F32)
    scale = lax.rsqrt(jnp.mean(x * x, axis=1, keepdims=True) + RMS_EPS)
    normed = (x * scale * gain_ref[...]).astype(BF16)
    n_ref[...] = normed
    low = jnp.dot(normed, low_ref[...], preferred_element_type=F32).astype(BF16)
    z = jnp.dot(low, high_ref[...], preferred_element_type=F32) + bias_ref[...]
    log_sig = jnp.minimum(z, 0.0) - jnp.log1p(jnp.exp(-jnp.abs(z)))
    d_ref[...] = log_sig / GATE_NORMALIZER + shift_ref[...]


def norm_and_decay(tokens, gain, low, high, bias, shift):
    rows, width = tokens.shape
    tile = rows // 6
    keys = high.shape[1]
    whole = lambda *shape: pl.BlockSpec(shape, lambda i: (0, 0))
    tiled = lambda cols: pl.BlockSpec((tile, cols), lambda i: (i, 0))
    return pl.pallas_call(
        norm_kernel,
        grid=(rows // tile,),
        in_specs=[
            tiled(width),
            whole(1, width),
            whole(*low.shape),
            whole(*high.shape),
            whole(1, keys),
            tiled(keys),
        ],
        out_specs=[tiled(width), tiled(keys)],
        out_shape=[
            jax.ShapeDtypeStruct((rows, width), BF16),
            jax.ShapeDtypeStruct((rows, keys), F32),
        ],
        cost_estimate=cost(rows * width * 64, rows * width * 4),
        name="norm",
    )(tokens, gain[None], low, high, bias[None], shift)


def project_kernel(x_ref, *refs, gated):
    *pieces, out_ref, weight = refs

    @pl.when(pl.program_id(0) == 0)
    def _():
        at = 0
        for piece in pieces:
            weight[at : at + piece.shape[0], :] = piece[...]
            at += piece.shape[0]

    product = jnp.dot(x_ref[...], weight[...], preferred_element_type=F32)
    if gated:
        half = product.shape[1] // 2
        product = product[:, :half] * jax.nn.sigmoid(product[:, half:])
    out_ref[...] = product.astype(out_ref.dtype)


def project(normed, pieces, gated):
    rows, depth = normed.shape
    cols = pieces[0].shape[1]
    tile = rows // 3
    out_cols = cols // 2 if gated else cols
    return pl.pallas_call(
        functools.partial(project_kernel, gated=gated),
        grid=(rows // tile,),
        in_specs=[pl.BlockSpec((tile, depth), lambda i: (i, 0))]
        + [pl.BlockSpec(piece.shape, lambda i: (0, 0)) for piece in pieces],
        out_specs=pl.BlockSpec((tile, out_cols), lambda i: (i, 0)),
        out_shape=jax.ShapeDtypeStruct((rows, out_cols), BF16),
        scratch_shapes=[pltpu.VMEM((depth, cols), BF16)],
        cost_estimate=cost(2 * rows * depth * cols, 2 * depth * (rows + cols)),
        name="project_gated" if gated else "project",
    )(normed, *pieces)


def dot_t(a, b):
    return lax.dot_general(a, b, (((1,), (1,)), ((), ())), preferred_element_type=F32)


def dot_rows(a, b):
    return lax.dot_general(a, b, (((0,), (0,)), ((), ())), preferred_element_type=F32)


def block_kernel(q_ref, k_ref, v_ref, d_ref, inner_ref, reach_ref, state_ref, total_ref, state, start):
    step = pl.program_id(0)

    @pl.when(step == 0)
    def _():
        state[...] = jnp.zeros_like(state)
        start[...] = jnp.zeros_like(start)

    size = d_ref.shape[0]
    row = lax.broadcasted_iota(jnp.int32, (size, size), 0)
    col = lax.broadcasted_iota(jnp.int32, (size, size), 1)
    lower = (row >= col).astype(F32)
    running = jnp.dot(
        lower, d_ref[...], precision=lax.Precision.HIGHEST, preferred_element_type=F32
    )
    final = running[size - 1 : size, :]
    before = start[0:1, :]
    q = q_ref[...].astype(F32) * DK ** (-0.5)
    k = k_ref[...].astype(F32)
    v = v_ref[...]
    scaled = q * jnp.exp(running)
    reach_ref[...] = (scaled * jnp.exp(before)).astype(BF16)
    scaled = scaled.astype(BF16)
    scores = dot_t(scaled, (k * jnp.exp(-running)).astype(BF16))
    scores = jnp.where(row >= col, scores, 0.0).astype(BF16)
    now = state[...]
    inner_ref[...] = jnp.dot(scores, v, preferred_element_type=F32) + dot_t(scaled, now.astype(BF16))
    later = jnp.exp(final) * now + dot_rows(v, (k * jnp.exp(final - running)).astype(BF16))
    state[...] = later
    start[0:1, :] = before + final

    @pl.when(step == pl.num_programs(0) - 1)
    def _():
        state_ref[...] = later.astype(BF16)
        total_ref[...] = jnp.exp(before + final)


def blocks(qkv, log_decay):
    rows = qkv.shape[0]
    part = lambda width, at: pl.BlockSpec((BLOCK, width), lambda i: (i, at))
    fixed = lambda *shape: pl.BlockSpec(shape, lambda i: (0, 0))
    return pl.pallas_call(
        block_kernel,
        grid=(rows // BLOCK,),
        in_specs=[part(DK, 0), part(DK, 1), part(DV, 1), part(DK, 0)],
        out_specs=[part(DV, 0), part(DK, 0), fixed(DV, DK), fixed(1, DK)],
        out_shape=[
            jax.ShapeDtypeStruct((rows, DV), F32),
            jax.ShapeDtypeStruct((rows, DK), BF16),
            jax.ShapeDtypeStruct((DV, DK), BF16),
            jax.ShapeDtypeStruct((1, DK), F32),
        ],
        scratch_shapes=[pltpu.VMEM((DV, DK), F32), pltpu.VMEM((8, DK), F32)],
        cost_estimate=cost(rows * DK * DV * 10, rows * 8192),
        name="blocks",
    )(qkv, qkv, qkv, log_decay)


def parted(a):
    high = a.astype(BF16)
    return high, (a - high.astype(F32)).astype(BF16)


def product(a, b, dims):
    dot = lambda x, y: lax.dot_general(x, y, (dims, ((), ())), preferred_element_type=F32)
    a_parts = (a,) if a.dtype == BF16 else parted(a)
    b_parts = (b,) if b.dtype == BF16 else parted(b)
    total = dot(a_parts[0], b_parts[0])
    if len(a_parts) > 1:
        total = total + dot(a_parts[1], b_parts[0])
    if len(b_parts) > 1:
        total = total + dot(a_parts[0], b_parts[1])
    return total


MESH = pl.DeviceIdType.MESH
A_B, B_A_T, A_T_B = ((1,), (0,)), ((1,), (1,)), ((0,), (0,))


def main_kernel(
    x_ref, gain_ref, low_ref, high_ref, bias_ref, shift_ref, own_a, own_b, own_c,
    inner_ref, reach_ref, state_ref, total_ref, glu_ref, far_ref,
    normed, decays, qkv, weight_a, weight_b, state, start,
    z_send, z_recv, f_send, f_recv, *, parts,
):
    place, column = lax.axis_index("sp"), lax.axis_index("fs")
    barrier = pltpu.get_barrier_semaphore()
    partners = [{"sp": lax.rem(place + s, parts)} for s in range(1, parts)]
    partners += [{"fs": column ^ 1}, {"fs": column ^ 2}]
    for partner in partners:
        pl.semaphore_signal(barrier, inc=1, device_id=partner, device_id_type=MESH)
    pl.semaphore_wait(barrier, len(partners))

    owns = (own_a, own_b, own_c)
    weights = (weight_a, weight_b)

    def along_z(g, s):
        rows = owns[g].shape[0] // 4
        source = owns[g].at[pl.ds(pl.multiple_of(column * rows, rows), rows), :]
        target = far_ref.at[s - 1] if g == 2 else weights[g].at[place * 4 + column]
        return pltpu.make_async_remote_copy(
            src_ref=source,
            dst_ref=target,
            send_sem=z_send.at[g, s - 1],
            recv_sem=z_recv.at[g, s - 1],
            device_id={"sp": lax.rem(place + s, parts)},
            device_id_type=MESH,
        )

    def along_f(g, s, way, mask, held):
        block = lax.rem(place - s + parts, parts) * 4 + (column ^ held)
        return pltpu.make_async_remote_copy(
            src_ref=weights[g].at[block],
            dst_ref=weights[g].at[block],
            send_sem=f_send.at[g, s - 1, way],
            recv_sem=f_recv.at[g, s - 1, way],
            device_id={"fs": column ^ mask},
            device_id_type=MESH,
        )

    def over_x(g, s):
        return along_f(g, s, 0, 1, 0)

    def over_y(g, s):
        return along_f(g, s, 1, 2, 0)

    def diagonal(g, s):
        return along_f(g, s, 2, 1, 2) if (s + g) % 2 else along_f(g, s, 2, 2, 1)

    def on_z(g):
        for s in range(1, parts):
            along_z(g, s).wait_recv()
            over_x(g, s).start()
            over_y(g, s).start()

    def on_f(g):
        for s in range(1, parts):
            over_x(g, s).wait_recv()
            over_y(g, s).wait_recv()
            diagonal(g, s).start()

    def on_diagonal(g):
        for s in range(1, parts):
            diagonal(g, s).wait_recv()

    for g in range(3):
        for s in range(1, parts):
            along_z(g, s).start()

    piece = own_a.shape[0] // 4
    for i in range(4):
        weight_a[place * 4 + i] = own_a[i * piece : (i + 1) * piece, :]
        weight_b[place * 4 + i] = own_b[i * piece : (i + 1) * piece, :]

    length = x_ref.shape[0]
    tile = length // 6

    def norm_tile(i, none):
        at = pl.ds(pl.multiple_of(i * tile, tile), tile)
        x = x_ref[at, :].astype(F32)
        scale = lax.rsqrt(jnp.mean(x * x, axis=1, keepdims=True) + RMS_EPS)
        rows = (x * scale * gain_ref[...]).astype(BF16)
        normed[at, :] = rows
        low = jnp.dot(rows, low_ref[...], preferred_element_type=F32).astype(BF16)
        z = jnp.dot(low, high_ref[...], preferred_element_type=F32) + bias_ref[...]
        log_sig = jnp.minimum(z, 0.0) - jnp.log1p(jnp.exp(-jnp.abs(z)))
        decays[at, :] = log_sig / GATE_NORMALIZER + shift_ref[at, :]
        return none

    lax.fori_loop(0, 6, norm_tile, 0)
    on_z(0)
    on_f(0)
    on_z(1)
    on_diagonal(0)

    def times(i, weight):
        at = pl.ds(pl.multiple_of(i * tile, tile), tile)
        full = weight[...].reshape(normed.shape[1], weight.shape[2])
        return at, jnp.dot(normed[at, :], full, preferred_element_type=F32)

    def qkv_tile(i, none):
        at, result = times(i, weight_a)
        qkv[at, :] = result.astype(BF16)
        return none

    lax.fori_loop(0, 6, qkv_tile, 0)

    state[...] = jnp.zeros_like(state)
    start[...] = jnp.zeros_like(start)
    row = lax.broadcasted_iota(jnp.int32, (BLOCK, BLOCK), 0)
    col = lax.broadcasted_iota(jnp.int32, (BLOCK, BLOCK), 1)

    def block_step(i, none):
        at = pl.ds(pl.multiple_of(i * BLOCK, BLOCK), BLOCK)
        lower = (row >= col).astype(BF16)
        decay = decays[at, :]
        high = decay.astype(BF16)
        rest = decay - high.astype(F32)
        middle = rest.astype(BF16)
        least = (rest - middle.astype(F32)).astype(BF16)
        running = (
            jnp.dot(lower, high, preferred_element_type=F32)
            + jnp.dot(lower, middle, preferred_element_type=F32)
            + jnp.dot(lower, least, preferred_element_type=F32)
        )
        final = running[BLOCK - 1 : BLOCK, :]
        before = start[0:1, :]
        q = qkv[at, 0:DK].astype(F32) * DK ** (-0.5)
        k = qkv[at, DK : 2 * DK].astype(F32)
        v = qkv[at, 2 * DK :]
        scaled = q * jnp.exp(running)
        reach_ref[at, :] = scaled * jnp.exp(before)
        scores = product(scaled, k * jnp.exp(-running), B_A_T)
        scores = jnp.where(row >= col, scores, 0.0)
        now = state[...]
        inner_ref[at, :] = product(scores, v, A_B) + product(scaled, now, B_A_T)
        update = product(v, k * jnp.exp(final - running), A_T_B)
        state[...] = jnp.exp(final) * now + update
        start[0:1, :] = before + final
        return none

    lax.fori_loop(0, length // BLOCK, block_step, 0)
    state_ref[...] = state[...].astype(BF16)
    total_ref[...] = jnp.exp(start[0:1, :])
    on_f(1)
    on_diagonal(1)

    def glu_tile(i, none):
        at, result = times(i, weight_b)
        half = result.shape[1] // 2
        glu_ref[at, :] = (result[:, :half] * jax.nn.sigmoid(result[:, half:])).astype(BF16)
        return none

    lax.fori_loop(0, 6, glu_tile, 0)
    for s in range(1, parts):
        along_z(2, s).wait_recv()
        for g in range(3):
            along_z(g, s).wait_send()
        for g in range(2):
            over_x(g, s).wait_send()
            over_y(g, s).wait_send()
            diagonal(g, s).wait_send()


def main_call(tokens, gain, low, high, bias, shift, own_a, own_b, own_c):
    parts = lax.axis_size("sp")
    rows, width = tokens.shape
    piece = own_a.shape[0] // 4
    vmem = pl.BlockSpec(memory_space=pltpu.VMEM)
    shape = jax.ShapeDtypeStruct
    return pl.pallas_call(
        functools.partial(main_kernel, parts=parts),
        in_specs=[vmem] * 9,
        out_specs=[vmem] * 6,
        out_shape=[
            shape((rows, DV), F32),
            shape((rows, DK), F32),
            shape((DV, DK), BF16),
            shape((1, DK), F32),
            shape((rows, own_b.shape[1] // 2), BF16),
            shape((parts - 1, own_c.shape[0] // 4, own_c.shape[1]), BF16),
        ],
        scratch_shapes=[
            pltpu.VMEM((rows, width), BF16),
            pltpu.VMEM((rows, DK), F32),
            pltpu.VMEM((rows, own_a.shape[1]), BF16),
            pltpu.VMEM((parts * 4, piece, own_a.shape[1]), BF16),
            pltpu.VMEM((parts * 4, piece, own_b.shape[1]), BF16),
            pltpu.VMEM((DV, DK), F32),
            pltpu.VMEM((8, DK), F32),
            pltpu.SemaphoreType.DMA((3, parts - 1)),
            pltpu.SemaphoreType.DMA((3, parts - 1)),
            pltpu.SemaphoreType.DMA((2, parts - 1, 3)),
            pltpu.SemaphoreType.DMA((2, parts - 1, 3)),
        ],
        compiler_params=pltpu.CompilerParams(
            collective_id=0, has_side_effects=True, vmem_limit_bytes=56 * 2**20
        ),
        cost_estimate=cost(40 * 10**9, 20 * 2**20),
        name="main",
    )(tokens, gain[None], low, high, bias[None], shift, own_a, own_b, own_c)


def finish_kernel(inner_ref, reach_ref, state_ref, gain_ref, out_ref):
    attended = inner_ref[...] + product(reach_ref[...], state_ref[...], B_A_T)
    mean_square = jnp.mean(attended * attended, axis=1, keepdims=True)
    out_ref[...] = (attended * lax.rsqrt(mean_square + RMS_EPS) * gain_ref[...]).astype(BF16)


def finish(inner, reach, state, gain):
    rows = inner.shape[0]
    tile = rows // 3
    tiled = lambda cols: pl.BlockSpec((tile, cols), lambda i: (i, 0))
    return pl.pallas_call(
        finish_kernel,
        grid=(rows // tile,),
        in_specs=[
            tiled(DV),
            tiled(DK),
            pl.BlockSpec((DV, DK), lambda i: (0, 0)),
            pl.BlockSpec((1, DV), lambda i: (0, 0)),
        ],
        out_specs=tiled(DV),
        out_shape=jax.ShapeDtypeStruct((rows, DV), BF16),
        cost_estimate=cost(rows * DK * DV * 2, rows * 4096),
        name="finish",
    )(inner, reach, state, gain[None])


def out_kernel(where, a_ref, c_ref, own_ref, *refs):
    far, over_x, over_y, first, second, out_ref, weight = refs
    depth, cols = own_ref.shape
    rows = depth // 4
    parts = far.shape[0] // rows + 1

    @pl.when(pl.program_id(0) == 0)
    def _():
        at = pl.multiple_of(where[1] * cols, cols)
        weight[:, pl.ds(at, cols)] = own_ref[...]
        for s in range(1, parts):
            at = pl.multiple_of(lax.rem(where[1] - s + parts, parts) * cols, cols)
            low = (s - 1) * rows
            cut = first.shape[0]
            sizes = [(far, low, rows, 0, 0), (over_x, low, rows, 1, 0), (over_y, low, rows, 2, 0)]
            end = low + rows
            if low < cut:
                sizes.append((first, low, min(end, cut) - low, 3, 0))
            if end > cut:
                begin = max(low, cut)
                sizes.append((second, begin - cut, end - begin, 3, begin - low))
            for source, begin, count, d, inside in sizes:
                to = pl.multiple_of((where[2] ^ d) * rows + inside, 128)
                weight[pl.ds(to, count), pl.ds(at, cols)] = source[begin : begin + count, :]

    half = depth // 2
    out_ref[...] = (
        jnp.dot(a_ref[...], weight[:half, :], preferred_element_type=F32)
        + jnp.dot(c_ref[...], weight[half:, :], preferred_element_type=F32)
    ).astype(out_ref.dtype)


def out_rows(where, attn, conv, own, pieces, dtype):
    rows, depth = attn.shape
    cols = own.shape[1] * lax.axis_size("sp")
    tile = rows // 6
    rowed = pl.BlockSpec((tile, depth), lambda i, w: (w[0] * 3 + i, 0))
    return pl.pallas_call(
        out_kernel,
        grid_spec=pltpu.PrefetchScalarGridSpec(
            num_scalar_prefetch=1,
            grid=(3,),
            in_specs=[rowed, rowed]
            + [pl.BlockSpec(piece.shape, lambda i, w: (0, 0)) for piece in (own, *pieces)],
            out_specs=pl.BlockSpec((tile, cols), lambda i, w: (i, 0)),
            scratch_shapes=[pltpu.VMEM((own.shape[0], cols), BF16)],
        ),
        out_shape=jax.ShapeDtypeStruct((rows // 2, cols), dtype),
        cost_estimate=cost(2 * rows * depth * cols, 4 * depth * cols),
        name="out_rows",
    )(where, attn, conv, own, *pieces)


def on_device(
    tokens,
    norm_gain,
    w_query,
    w_key,
    w_value,
    w_conv_value,
    w_conv_gate,
    w_decay_low,
    w_decay_high,
    gate_bias,
    decay_shift,
    head_gain,
    conv_taps,
    channel_gain,
    w_out_attn,
    w_out_conv,
    init_state,
):
    parts, turns = lax.axis_size("sp"), lax.axis_size("fs")
    place, column = lax.axis_index("sp"), lax.axis_index("fs")
    position = lax.axis_index("tp")
    direct = parts == 4 and turns == 4
    length_here = tokens.shape[1]
    key_cols = w_query.shape[1]
    conv_cols = w_conv_value.shape[1]
    own_qkv = jnp.concatenate([w_query, w_key, w_value], axis=1)
    own_conv = jnp.concatenate([w_conv_value, w_conv_gate], axis=1)
    own_out = jnp.concatenate([w_out_attn, w_out_conv], axis=0)
    high_cols = lax.dynamic_slice_in_dim(w_decay_high, position * key_cols, key_cols, 1)
    bias_here = lax.dynamic_slice_in_dim(gate_bias, position * key_cols, key_cols, 0)
    front = (tokens[0], norm_gain, w_decay_low, high_cols, bias_here, decay_shift[0])
    if direct:
        inner, reach, state, total, glu, far = main_call(*front, own_qkv, own_conv, own_out)
        far = far.reshape(-1, far.shape[2])
        over_x, over_y = swapped(far, 1), swapped(far, 2)
        cut = far.shape[0] // 2
        got_out = [far, over_x, over_y, swapped(over_y[:cut], 1), swapped(over_x[cut:], 2)]
    else:
        normed, log_decay = norm_and_decay(*front)
        qkv = project(normed, [gathered(own_qkv)], False)
        inner, reach, state, total = blocks(qkv, log_decay)
        glu = project(normed, [gathered(own_conv)], True)
        out_weight = lax.all_gather(own_out, "sp", axis=1, tiled=True)
    total_high = total.astype(BF16)
    total_low = (total - total_high.astype(F32)).astype(BF16)
    packed = jnp.concatenate([state, jnp.pad(total_high, ((0, 7), (0, 0))), jnp.pad(total_low, ((0, 7), (0, 0)))], axis=0)
    carried = jnp.zeros((DV, DK), F32)
    decay = jnp.ones((1, DK), F32)
    for s in range(1, parts):
        other = shifted(packed, "sp", s)
        carried = carried + decay * other[:DV].astype(F32)
        gone = other[DV : DV + 1].astype(F32) + other[DV + 8 : DV + 9].astype(F32)
        decay = decay * jnp.where(place >= s, gone, 1.0)
    incoming = carried + decay * init_state[0, 0].T
    attn_out = finish(inner, reach, incoming, head_gain)

    rim = shifted(glu[length_here - (KW - 1) :], "sp", 1)
    padded = jnp.concatenate([rim, glu], axis=0).astype(F32)
    taps_here = lax.dynamic_slice_in_dim(conv_taps, position * conv_cols, conv_cols, 1)
    filtered = jnp.zeros((length_here, conv_cols), F32)
    for tap_index in range(KW):
        filtered = filtered + taps_here[tap_index] * padded[tap_index : tap_index + length_here]
    first_sum, square_sum = lax.psum(
        (
            jnp.sum(filtered, axis=1, keepdims=True),
            jnp.sum(filtered * filtered, axis=1, keepdims=True),
        ),
        "tp",
    )
    mean = first_sum / CW
    centered = filtered - mean
    variance = square_sum / CW - mean * mean
    gain_here = lax.dynamic_slice_in_dim(channel_gain, position * conv_cols, conv_cols, 0)
    conv_out = jax.nn.silu(centered * lax.rsqrt(variance + LN_EPS) * gain_here).astype(BF16)

    if direct:
        at = lambda half: jnp.stack([half, place, column]).astype(jnp.int32)
        given = out_rows(at(1 - position), attn_out, conv_out, own_out, got_out, BF16)
        taken = lax.ppermute(given, "tp", [(0, 1), (1, 0)])
        kept = out_rows(at(position), attn_out, conv_out, own_out, got_out, F32)
    else:
        both = jnp.concatenate([attn_out, conv_out], axis=1)
        columns = jnp.dot(both, out_weight, preferred_element_type=F32)
        half = length_here // 2
        kept = lax.dynamic_slice_in_dim(columns, position * half, half, 0)
        given = lax.dynamic_slice_in_dim(columns, (1 - position) * half, half, 0).astype(BF16)
        taken = lax.ppermute(given, "tp", [(0, 1), (1, 0)])
    return (kept + taken.astype(F32)).astype(BF16)[None]


def solution(mesh):
    in_specs = (
        P("fs", "sp", None),
        P(),
        P("sp", "tp"),
        P("sp", "tp"),
        P("sp", "tp"),
        P("sp", "tp"),
        P("sp", "tp"),
        P(),
        P(),
        P(),
        P("fs", "sp", "tp"),
        P(),
        P(),
        P(),
        P("tp", "sp"),
        P("tp", "sp"),
        P("fs", "tp", None, None),
    )
    out_specs = P("fs", ("sp", "tp"), None)
    return jax.shard_map(
        on_device, mesh=mesh, in_specs=in_specs, out_specs=out_specs, check_vma=False
    )
```

```python
import functools

import jax
import jax.numpy as jnp
from jax import lax
from jax.experimental import pallas as pl
from jax.experimental.pallas import tpu as pltpu
from jax.sharding import PartitionSpec as P

DK = 256
DV = 512
CW = 1024
KW = 31
BLOCK = 64


RMS_EPS = 1e-06
LN_EPS = 1e-05
GATE_NORMALIZER = 16.0
F32 = jnp.float32
BF16 = jnp.bfloat16


def cost(flops, nbytes):
    return pl.CostEstimate(flops=flops, bytes_accessed=nbytes, transcendentals=0)


def shifted(value, axis, steps):
    count = lax.axis_size(axis)
    initial, last = (max(0, -steps), min(count, count - steps))
    return lax.ppermute(value, axis, [(source, source + steps) for source in range(initial, last)])


def gathered(own):
    rows = own.shape[0] // lax.axis_size("fs")
    piece = lax.dynamic_slice_in_dim(own, lax.axis_index("fs") * rows, rows, 0)
    return lax.all_gather(piece, ("sp", "fs"), axis=0, tiled=True)


def norm_kernel(x_ref, gain_ref, low_ref, high_ref, bias_ref, shift_ref, n_ref, d_ref):
    x = x_ref[...].astype(F32)
    scale = lax.rsqrt(jnp.mean(x * x, axis=1, keepdims=True) + RMS_EPS)
    normed = (x * scale * gain_ref[...]).astype(BF16)
    n_ref[...] = normed
    low = jnp.dot(normed, low_ref[...], preferred_element_type=F32).astype(BF16)
    z = jnp.dot(low, high_ref[...], preferred_element_type=F32) + bias_ref[...]
    log_sig = jnp.minimum(z, 0.0) - jnp.log1p(jnp.exp(-jnp.abs(z)))
    d_ref[...] = log_sig / GATE_NORMALIZER + shift_ref[...]


def norm_and_decay(tokens, gain, low, high, bias, shift):
    rows, width = tokens.shape
    tile = rows // 6
    keys = high.shape[1]
    whole = lambda *shape: pl.BlockSpec(shape, lambda i: (0, 0))
    tiled = lambda cols: pl.BlockSpec((tile, cols), lambda i: (i, 0))
    return pl.pallas_call(
        norm_kernel,
        grid=(rows // tile,),
        in_specs=[
            tiled(width),
            whole(1, width),
            whole(*low.shape),
            whole(*high.shape),
            whole(1, keys),
            tiled(keys),
        ],
        out_specs=[tiled(width), tiled(keys)],
        out_shape=[
            jax.ShapeDtypeStruct((rows, width), BF16),
            jax.ShapeDtypeStruct((rows, keys), F32),
        ],
        cost_estimate=cost(rows * width * 64, rows * width * 4),
        name="norm",
    )(tokens, gain[None], low, high, bias[None], shift)


def project_kernel(x_ref, *refs, gated):
    *pieces, out_ref, weight = refs

    @pl.when(pl.program_id(0) == 0)
    def _():
        at = 0
        for piece in pieces:
            weight[at : at + piece.shape[0], :] = piece[...]
            at += piece.shape[0]

    product = jnp.dot(x_ref[...], weight[...], preferred_element_type=F32)
    if gated:
        half = product.shape[1] // 2
        product = product[:, :half] * jax.nn.sigmoid(product[:, half:])
    out_ref[...] = product.astype(out_ref.dtype)


def project(normed, pieces, gated):
    rows, depth = normed.shape
    cols = pieces[0].shape[1]
    tile = rows // 3
    out_cols = cols // 2 if gated else cols
    return pl.pallas_call(
        functools.partial(project_kernel, gated=gated),
        grid=(rows // tile,),
        in_specs=[pl.BlockSpec((tile, depth), lambda i: (i, 0))]
        + [pl.BlockSpec(piece.shape, lambda i: (0, 0)) for piece in pieces],
        out_specs=pl.BlockSpec((tile, out_cols), lambda i: (i, 0)),
        out_shape=jax.ShapeDtypeStruct((rows, out_cols), BF16),
        scratch_shapes=[pltpu.VMEM((depth, cols), BF16)],
        cost_estimate=cost(2 * rows * depth * cols, 2 * depth * (rows + cols)),
        name="project_gated" if gated else "project",
    )(normed, *pieces)


def dot_t(a, b):
    return lax.dot_general(a, b, (((1,), (1,)), ((), ())), preferred_element_type=F32)


def dot_rows(a, b):
    return lax.dot_general(a, b, (((0,), (0,)), ((), ())), preferred_element_type=F32)


def block_kernel(q_ref, k_ref, v_ref, d_ref, inner_ref, reach_ref, state_ref, total_ref, state, start):
    step = pl.program_id(0)

    @pl.when(step == 0)
    def _():
        state[...] = jnp.zeros_like(state)
        start[...] = jnp.zeros_like(start)

    size = d_ref.shape[0]
    row = lax.broadcasted_iota(jnp.int32, (size, size), 0)
    col = lax.broadcasted_iota(jnp.int32, (size, size), 1)
    lower = (row >= col).astype(F32)
    running = jnp.dot(
        lower, d_ref[...], precision=lax.Precision.HIGHEST, preferred_element_type=F32
    )
    final = running[size - 1 : size, :]
    before = start[0:1, :]
    q = q_ref[...].astype(F32) * DK ** (-0.5)
    k = k_ref[...].astype(F32)
    v = v_ref[...]
    scaled = q * jnp.exp(running)
    reach_ref[...] = (scaled * jnp.exp(before)).astype(BF16)
    scaled = scaled.astype(BF16)
    scores = dot_t(scaled, (k * jnp.exp(-running)).astype(BF16))
    scores = jnp.where(row >= col, scores, 0.0).astype(BF16)
    now = state[...]
    inner_ref[...] = jnp.dot(scores, v, preferred_element_type=F32) + dot_t(scaled, now.astype(BF16))
    later = jnp.exp(final) * now + dot_rows(v, (k * jnp.exp(final - running)).astype(BF16))
    state[...] = later
    start[0:1, :] = before + final

    @pl.when(step == pl.num_programs(0) - 1)
    def _():
        state_ref[...] = later.astype(BF16)
        total_ref[...] = jnp.exp(before + final)


def blocks(qkv, log_decay):
    rows = qkv.shape[0]
    part = lambda width, at: pl.BlockSpec((BLOCK, width), lambda i: (i, at))
    fixed = lambda *shape: pl.BlockSpec(shape, lambda i: (0, 0))
    return pl.pallas_call(
        block_kernel,
        grid=(rows // BLOCK,),
        in_specs=[part(DK, 0), part(DK, 1), part(DV, 1), part(DK, 0)],
        out_specs=[part(DV, 0), part(DK, 0), fixed(DV, DK), fixed(1, DK)],
        out_shape=[
            jax.ShapeDtypeStruct((rows, DV), F32),
            jax.ShapeDtypeStruct((rows, DK), BF16),
            jax.ShapeDtypeStruct((DV, DK), BF16),
            jax.ShapeDtypeStruct((1, DK), F32),
        ],
        scratch_shapes=[pltpu.VMEM((DV, DK), F32), pltpu.VMEM((8, DK), F32)],
        cost_estimate=cost(rows * DK * DV * 10, rows * 8192),
        name="blocks",
    )(qkv, qkv, qkv, log_decay)


def parted(a):
    high = a.astype(BF16)
    return high, (a - high.astype(F32)).astype(BF16)


def product(a, b, dims):
    dot = lambda x, y: lax.dot_general(x, y, (dims, ((), ())), preferred_element_type=F32)
    a_parts = (a,) if a.dtype == BF16 else parted(a)
    b_parts = (b,) if b.dtype == BF16 else parted(b)
    total = dot(a_parts[0], b_parts[0])
    if len(a_parts) > 1:
        total = total + dot(a_parts[1], b_parts[0])
    if len(b_parts) > 1:
        total = total + dot(a_parts[0], b_parts[1])
    return total


MESH = pl.DeviceIdType.MESH
A_B, B_A_T, A_T_B = ((1,), (0,)), ((1,), (1,)), ((0,), (0,))


def main_kernel(
    x_ref, gain_ref, low_ref, high_ref, bias_ref, shift_ref, own_a, own_b, own_c,
    inner_ref, reach_ref, far_state, glu_ref, far_rim, weight_c,
    normed, decays, qkv, weight_a, weight_b, state, start, packed,
    z_send, z_recv, f_send, f_recv, s_send, s_recv, r_send, r_recv, *, parts,
):
    place, column = lax.axis_index("sp"), lax.axis_index("fs")
    position = lax.axis_index("tp")
    barrier = pltpu.get_barrier_semaphore()
    partners = [{"sp": lax.rem(place + s, parts)} for s in range(1, parts)]
    partners += [{"fs": column ^ 1}, {"fs": column ^ 2}]
    for partner in partners:
        pl.semaphore_signal(barrier, inc=1, device_id=partner, device_id_type=MESH)
    pl.semaphore_wait(barrier, len(partners))

    owns = (own_a, own_b, own_c)
    weights = (weight_a, weight_b, weight_c)

    def along_z(g, s):
        rows = owns[g].shape[0] // 4
        source = owns[g].at[pl.ds(pl.multiple_of(column * rows, rows), rows), :]
        target = weights[g].at[place * 4 + column]
        return pltpu.make_async_remote_copy(
            src_ref=source,
            dst_ref=target,
            send_sem=z_send.at[g, s - 1],
            recv_sem=z_recv.at[g, s - 1],
            device_id={"sp": lax.rem(place + s, parts)},
            device_id_type=MESH,
        )

    def along_f(g, s, way, mask, held):
        block = lax.rem(place - s + parts, parts) * 4 + (column ^ held)
        return pltpu.make_async_remote_copy(
            src_ref=weights[g].at[block],
            dst_ref=weights[g].at[block],
            send_sem=f_send.at[g, s - 1, way],
            recv_sem=f_recv.at[g, s - 1, way],
            device_id={"fs": column ^ mask},
            device_id_type=MESH,
        )

    def over_x(g, s):
        return along_f(g, s, 0, 1, 0)

    def over_y(g, s):
        return along_f(g, s, 1, 2, 0)

    def diagonal(g, s):
        return along_f(g, s, 2, 1, 2) if (s + g) % 2 else along_f(g, s, 2, 2, 1)

    def on_z(g):
        for s in range(1, parts):
            along_z(g, s).wait_recv()
            over_x(g, s).start()
            over_y(g, s).start()

    def on_f(g):
        for s in range(1, parts):
            over_x(g, s).wait_recv()
            over_y(g, s).wait_recv()
            diagonal(g, s).start()

    def on_diagonal(g):
        for s in range(1, parts):
            diagonal(g, s).wait_recv()

    def state_to(s):
        return pltpu.make_async_remote_copy(
            src_ref=packed,
            dst_ref=far_state.at[s - 1],
            send_sem=s_send.at[s - 1],
            recv_sem=s_recv.at[s - 1],
            device_id={"sp": lax.rem(place + s, parts)},
            device_id_type=MESH,
        )

    def rim_to():
        edge = far_rim.shape[0]
        return pltpu.make_async_remote_copy(
            src_ref=glu_ref.at[glu_ref.shape[0] - edge :, :],
            dst_ref=far_rim,
            send_sem=r_send,
            recv_sem=r_recv,
            device_id={"sp": lax.rem(place + 1, parts)},
            device_id_type=MESH,
        )

    def z_start(g):
        for s in range(1, parts):
            along_z(g, s).start()

    z_start(0)
    for own, weight in zip(owns, weights):
        piece = own.shape[0] // 4
        for i in range(4):
            weight[place * 4 + i] = own[i * piece : (i + 1) * piece, :]

    length = x_ref.shape[0]
    tile = length // 3
    keys = shift_ref.shape[1]
    mine = pl.ds(pl.multiple_of(position * keys, keys), keys)

    def norm_tile(i, none):
        at = pl.ds(pl.multiple_of(i * tile, tile), tile)
        x = x_ref[at, :].astype(F32)
        scale = lax.rsqrt(jnp.mean(x * x, axis=1, keepdims=True) + RMS_EPS)
        rows = (x * scale * gain_ref[...]).astype(BF16)
        normed[at, :] = rows
        low = jnp.dot(rows, low_ref[...], preferred_element_type=F32).astype(BF16)
        z = jnp.dot(low, high_ref[:, mine], preferred_element_type=F32) + bias_ref[:, mine]
        log_sig = jnp.minimum(z, 0.0) - jnp.log1p(jnp.exp(-jnp.abs(z)))
        decays[at, :] = log_sig / GATE_NORMALIZER + shift_ref[at, :]
        return none

    lax.fori_loop(0, 3, norm_tile, 0)
    on_z(0)
    z_start(1)
    on_f(0)
    on_z(1)
    z_start(2)
    on_diagonal(0)

    def times(i, weight):
        at = pl.ds(pl.multiple_of(i * tile, tile), tile)
        full = weight[...].reshape(normed.shape[1], weight.shape[2])
        return at, jnp.dot(normed[at, :], full, preferred_element_type=F32)

    def qkv_tile(i, none):
        at, result = times(i, weight_a)
        qkv[at, :] = result.astype(BF16)
        return none

    lax.fori_loop(0, 3, qkv_tile, 0)

    state[...] = jnp.zeros_like(state)
    start[...] = jnp.zeros_like(start)
    row = lax.broadcasted_iota(jnp.int32, (BLOCK, BLOCK), 0)
    col = lax.broadcasted_iota(jnp.int32, (BLOCK, BLOCK), 1)

    def block_step(i, none):
        at = pl.ds(pl.multiple_of(i * BLOCK, BLOCK), BLOCK)
        lower = (row >= col).astype(BF16)
        decay = decays[at, :]
        high = decay.astype(BF16)
        rest = decay - high.astype(F32)
        middle = rest.astype(BF16)
        least = (rest - middle.astype(F32)).astype(BF16)
        running = (
            jnp.dot(lower, high, preferred_element_type=F32)
            + jnp.dot(lower, middle, preferred_element_type=F32)
            + jnp.dot(lower, least, preferred_element_type=F32)
        )
        final = running[BLOCK - 1 : BLOCK, :]
        before = start[0:1, :]
        q = qkv[at, 0:DK].astype(F32) * DK ** (-0.5)
        k = qkv[at, DK : 2 * DK].astype(F32)
        v = qkv[at, 2 * DK :]
        scaled = q * jnp.exp(running)
        reach_ref[at, :] = scaled * jnp.exp(before)
        scores = product(scaled, k * jnp.exp(-running), B_A_T)
        scores = jnp.where(row >= col, scores, 0.0)
        now = state[...]
        inner_ref[at, :] = product(scores, v, A_B) + product(scaled, now, B_A_T)
        update = product(v, k * jnp.exp(final - running), A_T_B)
        state[...] = jnp.exp(final) * now + update
        start[0:1, :] = before + final
        return none

    count = length // BLOCK
    lax.fori_loop(0, count // 2, block_step, 0)
    on_f(1)
    lax.fori_loop(count // 2, count, block_step, 0)
    total = jnp.exp(start[0:1, :])
    high, low = parted(total)
    width = packed.shape[1]
    packed[:DV, :] = state[...].astype(BF16)
    packed[DV:, :] = jnp.concatenate(
        [
            jnp.broadcast_to(high.astype(F32), (8, width)),
            jnp.broadcast_to(low.astype(F32), (8, width)),
        ],
        axis=0,
    ).astype(BF16)
    on_z(2)
    on_diagonal(1)
    for s in range(1, parts):
        state_to(s).start()

    def glu_tile(i, none):
        at, result = times(i, weight_b)
        half = result.shape[1] // 2
        glu_ref[at, :] = (result[:, :half] * jax.nn.sigmoid(result[:, half:])).astype(BF16)
        return none

    lax.fori_loop(0, 3, glu_tile, 0)
    on_f(2)
    rim_to().start()
    on_diagonal(2)
    rim_to().wait()
    for s in range(1, parts):
        state_to(s).wait()
        for g in range(3):
            along_z(g, s).wait_send()
            over_x(g, s).wait_send()
            over_y(g, s).wait_send()
            diagonal(g, s).wait_send()


def main_call(tokens, gain, low, high, bias, shift, own_a, own_b, own_c):
    parts = lax.axis_size("sp")
    rows, width = tokens.shape
    piece = own_a.shape[0] // 4
    vmem = pl.BlockSpec(memory_space=pltpu.VMEM)
    shape = jax.ShapeDtypeStruct
    return pl.pallas_call(
        functools.partial(main_kernel, parts=parts),
        in_specs=[vmem] * 9,
        out_specs=[vmem] * 6,
        out_shape=[
            shape((rows, DV), F32),
            shape((rows, DK), F32),
            shape((parts - 1, DV + 16, DK), BF16),
            shape((rows, own_b.shape[1] // 2), BF16),
            shape((32, own_b.shape[1] // 2), BF16),
            shape((parts * 4, own_c.shape[0] // 4, own_c.shape[1]), BF16),
        ],
        scratch_shapes=[
            pltpu.VMEM((rows, width), BF16),
            pltpu.VMEM((rows, DK), F32),
            pltpu.VMEM((rows, own_a.shape[1]), BF16),
            pltpu.VMEM((parts * 4, piece, own_a.shape[1]), BF16),
            pltpu.VMEM((parts * 4, piece, own_b.shape[1]), BF16),
            pltpu.VMEM((DV, DK), F32),
            pltpu.VMEM((8, DK), F32),
            pltpu.VMEM((DV + 16, DK), BF16),
            pltpu.SemaphoreType.DMA((3, parts - 1)),
            pltpu.SemaphoreType.DMA((3, parts - 1)),
            pltpu.SemaphoreType.DMA((3, parts - 1, 3)),
            pltpu.SemaphoreType.DMA((3, parts - 1, 3)),
            pltpu.SemaphoreType.DMA((parts - 1,)),
            pltpu.SemaphoreType.DMA((parts - 1,)),
            pltpu.SemaphoreType.DMA,
            pltpu.SemaphoreType.DMA,
        ],
        compiler_params=pltpu.CompilerParams(
            collective_id=0, has_side_effects=True, vmem_limit_bytes=56 * 2**20
        ),
        cost_estimate=cost(40 * 10**9, 20 * 2**20),
        name="main",
    )(tokens, gain[None], low, high, bias[None], shift, own_a, own_b, own_c)


def finish_kernel(inner_ref, reach_ref, state_ref, gain_ref, out_ref):
    attended = inner_ref[...] + product(reach_ref[...], state_ref[...], B_A_T)
    mean_square = jnp.mean(attended * attended, axis=1, keepdims=True)
    out_ref[...] = (attended * lax.rsqrt(mean_square + RMS_EPS) * gain_ref[...]).astype(BF16)


def finish(inner, reach, state, gain):
    rows = inner.shape[0]
    tile = rows // 3
    tiled = lambda cols: pl.BlockSpec((tile, cols), lambda i: (i, 0))
    return pl.pallas_call(
        finish_kernel,
        grid=(rows // tile,),
        in_specs=[
            tiled(DV),
            tiled(DK),
            pl.BlockSpec((DV, DK), lambda i: (0, 0)),
            pl.BlockSpec((1, DV), lambda i: (0, 0)),
        ],
        out_specs=tiled(DV),
        out_shape=jax.ShapeDtypeStruct((rows, DV), BF16),
        cost_estimate=cost(rows * DK * DV * 2, rows * 4096),
        name="finish",
    )(inner, reach, state, gain[None])


def out_kernel(where, a_ref, c_ref, weight_ref, out_ref):
    half = weight_ref.shape[1] // 2
    out_ref[...] = (
        jnp.dot(a_ref[...], weight_ref[0, :half, :], preferred_element_type=F32)
        + jnp.dot(c_ref[...], weight_ref[0, half:, :], preferred_element_type=F32)
    ).astype(out_ref.dtype)


def out_rows(where, attn, conv, weight, dtype):
    rows, depth = attn.shape
    parts, both, cols = weight.shape
    half = rows // 2
    rowed = pl.BlockSpec((half, depth), lambda z, w: (w[0], 0))
    return pl.pallas_call(
        out_kernel,
        grid_spec=pltpu.PrefetchScalarGridSpec(
            num_scalar_prefetch=1,
            grid=(parts,),
            in_specs=[rowed, rowed, pl.BlockSpec((1, both, cols), lambda z, w: (z, 0, 0))],
            out_specs=pl.BlockSpec((half, cols), lambda z, w: (0, z)),
        ),
        out_shape=jax.ShapeDtypeStruct((half, parts * cols), dtype),
        cost_estimate=cost(2 * half * both * cols * parts, 4 * both * cols * parts),
        name="out_rows",
    )(where, attn, conv, weight)


def on_device(
    tokens,
    norm_gain,
    w_query,
    w_key,
    w_value,
    w_conv_value,
    w_conv_gate,
    w_decay_low,
    w_decay_high,
    gate_bias,
    decay_shift,
    head_gain,
    conv_taps,
    channel_gain,
    w_out_attn,
    w_out_conv,
    init_state,
):
    parts, turns = lax.axis_size("sp"), lax.axis_size("fs")
    place, position = lax.axis_index("sp"), lax.axis_index("tp")
    direct = parts == 4 and turns == 4
    length_here = tokens.shape[1]
    key_cols = w_query.shape[1]
    conv_cols = w_conv_value.shape[1]
    own_qkv = jnp.concatenate([w_query, w_key, w_value], axis=1)
    own_conv = jnp.concatenate([w_conv_value, w_conv_gate], axis=1)
    own_out = jnp.concatenate([w_out_attn, w_out_conv], axis=0)
    if direct:
        inner, reach, others, glu, rim, out_weight = main_call(
            tokens[0],
            norm_gain,
            w_decay_low,
            w_decay_high,
            gate_bias,
            decay_shift[0],
            own_qkv,
            own_conv,
            own_out,
        )
        out_weight = out_weight.reshape(parts, -1, out_weight.shape[2])
    else:
        high_cols = lax.dynamic_slice_in_dim(w_decay_high, position * key_cols, key_cols, 1)
        bias_here = lax.dynamic_slice_in_dim(gate_bias, position * key_cols, key_cols, 0)
        normed, log_decay = norm_and_decay(
            tokens[0], norm_gain, w_decay_low, high_cols, bias_here, decay_shift[0]
        )
        qkv = project(normed, [gathered(own_qkv)], False)
        inner, reach, state, total = blocks(qkv, log_decay)
        high, low = parted(total)
        edges = [jnp.broadcast_to(part, (8, DK)) for part in (high, low)]
        packed = jnp.concatenate([state, *edges], axis=0)
        others = [shifted(packed, "sp", s) for s in range(1, parts)]
        glu = project(normed, [gathered(own_conv)], True)
        rim = shifted(glu[length_here - 32 :], "sp", 1)
        out_weight = lax.all_gather(own_out, "sp", axis=1, tiled=True)
    carried = jnp.zeros((DV, DK), F32)
    decay = jnp.ones((1, DK), F32)
    for s in range(1, parts):
        other = others[s - 1].astype(F32)
        gone = other[DV : DV + 1] + other[DV + 8 : DV + 9]
        carried = carried + jnp.where(place >= s, decay * other[:DV], 0.0)
        decay = decay * jnp.where(place >= s, gone, 1.0)
    incoming = carried + decay * init_state[0, 0].T
    attn_out = finish(inner, reach, incoming, head_gain)

    rim = jnp.where(place >= 1, rim[rim.shape[0] - (KW - 1) :], jnp.zeros((), BF16))
    padded = jnp.concatenate([rim, glu], axis=0).astype(F32)
    taps_here = lax.dynamic_slice_in_dim(conv_taps, position * conv_cols, conv_cols, 1)
    filtered = jnp.zeros((length_here, conv_cols), F32)
    for tap_index in range(KW):
        filtered = filtered + taps_here[tap_index] * padded[tap_index : tap_index + length_here]
    first_sum, square_sum = lax.psum(
        (
            jnp.sum(filtered, axis=1, keepdims=True),
            jnp.sum(filtered * filtered, axis=1, keepdims=True),
        ),
        "tp",
    )
    mean = first_sum / CW
    centered = filtered - mean
    variance = square_sum / CW - mean * mean
    gain_here = lax.dynamic_slice_in_dim(channel_gain, position * conv_cols, conv_cols, 0)
    conv_out = jax.nn.silu(centered * lax.rsqrt(variance + LN_EPS) * gain_here).astype(BF16)

    if direct:
        at = lambda half: half.astype(jnp.int32)[None]
        given = out_rows(at(1 - position), attn_out, conv_out, out_weight, BF16)
        taken = lax.ppermute(given, "tp", [(0, 1), (1, 0)])
        kept = out_rows(at(position), attn_out, conv_out, out_weight, F32)
    else:
        both = jnp.concatenate([attn_out, conv_out], axis=1)
        columns = jnp.dot(both, out_weight, preferred_element_type=F32)
        half = length_here // 2
        kept = lax.dynamic_slice_in_dim(columns, position * half, half, 0)
        given = lax.dynamic_slice_in_dim(columns, (1 - position) * half, half, 0).astype(BF16)
        taken = lax.ppermute(given, "tp", [(0, 1), (1, 0)])
    return (kept + taken.astype(F32)).astype(BF16)[None]


def solution(mesh):
    in_specs = (
        P("fs", "sp", None),
        P(),
        P("sp", "tp"),
        P("sp", "tp"),
        P("sp", "tp"),
        P("sp", "tp"),
        P("sp", "tp"),
        P(),
        P(),
        P(),
        P("fs", "sp", "tp"),
        P(),
        P(),
        P(),
        P("tp", "sp"),
        P("tp", "sp"),
        P("fs", "tp", None, None),
    )
    out_specs = P("fs", ("sp", "tp"), None)
    return jax.shard_map(
        on_device, mesh=mesh, in_specs=in_specs, out_specs=out_specs, check_vma=False
    )
```

```python
import functools

import jax
import jax.numpy as jnp
from jax import lax
from jax.experimental import pallas as pl
from jax.experimental.pallas import tpu as pltpu
from jax.sharding import PartitionSpec as P

DK = 256
DV = 512
CW = 1024
KW = 31
BLOCK = 64


RMS_EPS = 1e-06
LN_EPS = 1e-05
GATE_NORMALIZER = 16.0
F32 = jnp.float32
BF16 = jnp.bfloat16


def cost(flops, nbytes):
    return pl.CostEstimate(flops=flops, bytes_accessed=nbytes, transcendentals=0)


def shifted(value, axis, steps):
    count = lax.axis_size(axis)
    initial, last = (max(0, -steps), min(count, count - steps))
    return lax.ppermute(value, axis, [(source, source + steps) for source in range(initial, last)])


def gathered(own):
    rows = own.shape[0] // lax.axis_size("fs")
    piece = lax.dynamic_slice_in_dim(own, lax.axis_index("fs") * rows, rows, 0)
    return lax.all_gather(piece, ("sp", "fs"), axis=0, tiled=True)


def norm_kernel(x_ref, gain_ref, low_ref, high_ref, bias_ref, shift_ref, n_ref, d_ref):
    x = x_ref[...].astype(F32)
    scale = lax.rsqrt(jnp.mean(x * x, axis=1, keepdims=True) + RMS_EPS)
    normed = (x * scale * gain_ref[...]).astype(BF16)
    n_ref[...] = normed
    low = jnp.dot(normed, low_ref[...], preferred_element_type=F32).astype(BF16)
    z = jnp.dot(low, high_ref[...], preferred_element_type=F32) + bias_ref[...]
    log_sig = jnp.minimum(z, 0.0) - jnp.log1p(jnp.exp(-jnp.abs(z)))
    d_ref[...] = log_sig / GATE_NORMALIZER + shift_ref[...]


def norm_and_decay(tokens, gain, low, high, bias, shift):
    rows, width = tokens.shape
    tile = rows // 6
    keys = high.shape[1]
    whole = lambda *shape: pl.BlockSpec(shape, lambda i: (0, 0))
    tiled = lambda cols: pl.BlockSpec((tile, cols), lambda i: (i, 0))
    return pl.pallas_call(
        norm_kernel,
        grid=(rows // tile,),
        in_specs=[
            tiled(width),
            whole(1, width),
            whole(*low.shape),
            whole(*high.shape),
            whole(1, keys),
            tiled(keys),
        ],
        out_specs=[tiled(width), tiled(keys)],
        out_shape=[
            jax.ShapeDtypeStruct((rows, width), BF16),
            jax.ShapeDtypeStruct((rows, keys), F32),
        ],
        cost_estimate=cost(rows * width * 64, rows * width * 4),
        name="norm",
    )(tokens, gain[None], low, high, bias[None], shift)


def project_kernel(x_ref, *refs, gated):
    *pieces, out_ref, weight = refs

    @pl.when(pl.program_id(0) == 0)
    def _():
        at = 0
        for piece in pieces:
            weight[at : at + piece.shape[0], :] = piece[...]
            at += piece.shape[0]

    product = jnp.dot(x_ref[...], weight[...], preferred_element_type=F32)
    if gated:
        half = product.shape[1] // 2
        product = product[:, :half] * jax.nn.sigmoid(product[:, half:])
    out_ref[...] = product.astype(out_ref.dtype)


def project(normed, pieces, gated):
    rows, depth = normed.shape
    cols = pieces[0].shape[1]
    tile = rows // 3
    out_cols = cols // 2 if gated else cols
    return pl.pallas_call(
        functools.partial(project_kernel, gated=gated),
        grid=(rows // tile,),
        in_specs=[pl.BlockSpec((tile, depth), lambda i: (i, 0))]
        + [pl.BlockSpec(piece.shape, lambda i: (0, 0)) for piece in pieces],
        out_specs=pl.BlockSpec((tile, out_cols), lambda i: (i, 0)),
        out_shape=jax.ShapeDtypeStruct((rows, out_cols), BF16),
        scratch_shapes=[pltpu.VMEM((depth, cols), BF16)],
        cost_estimate=cost(2 * rows * depth * cols, 2 * depth * (rows + cols)),
        name="project_gated" if gated else "project",
    )(normed, *pieces)


def dot_t(a, b):
    return lax.dot_general(a, b, (((1,), (1,)), ((), ())), preferred_element_type=F32)


def dot_rows(a, b):
    return lax.dot_general(a, b, (((0,), (0,)), ((), ())), preferred_element_type=F32)


def block_kernel(q_ref, k_ref, v_ref, d_ref, inner_ref, reach_ref, state_ref, total_ref, state, start):
    step = pl.program_id(0)

    @pl.when(step == 0)
    def _():
        state[...] = jnp.zeros_like(state)
        start[...] = jnp.zeros_like(start)

    size = d_ref.shape[0]
    row = lax.broadcasted_iota(jnp.int32, (size, size), 0)
    col = lax.broadcasted_iota(jnp.int32, (size, size), 1)
    lower = (row >= col).astype(F32)
    running = jnp.dot(
        lower, d_ref[...], precision=lax.Precision.HIGHEST, preferred_element_type=F32
    )
    final = running[size - 1 : size, :]
    before = start[0:1, :]
    q = q_ref[...].astype(F32) * DK ** (-0.5)
    k = k_ref[...].astype(F32)
    v = v_ref[...]
    scaled = q * jnp.exp(running)
    reach_ref[...] = (scaled * jnp.exp(before)).astype(BF16)
    scaled = scaled.astype(BF16)
    scores = dot_t(scaled, (k * jnp.exp(-running)).astype(BF16))
    scores = jnp.where(row >= col, scores, 0.0).astype(BF16)
    now = state[...]
    inner_ref[...] = jnp.dot(scores, v, preferred_element_type=F32) + dot_t(scaled, now.astype(BF16))
    later = jnp.exp(final) * now + dot_rows(v, (k * jnp.exp(final - running)).astype(BF16))
    state[...] = later
    start[0:1, :] = before + final

    @pl.when(step == pl.num_programs(0) - 1)
    def _():
        state_ref[...] = later.astype(BF16)
        total_ref[...] = jnp.exp(before + final)


def blocks(qkv, log_decay):
    rows = qkv.shape[0]
    part = lambda width, at: pl.BlockSpec((BLOCK, width), lambda i: (i, at))
    fixed = lambda *shape: pl.BlockSpec(shape, lambda i: (0, 0))
    return pl.pallas_call(
        block_kernel,
        grid=(rows // BLOCK,),
        in_specs=[part(DK, 0), part(DK, 1), part(DV, 1), part(DK, 0)],
        out_specs=[part(DV, 0), part(DK, 0), fixed(DV, DK), fixed(1, DK)],
        out_shape=[
            jax.ShapeDtypeStruct((rows, DV), F32),
            jax.ShapeDtypeStruct((rows, DK), BF16),
            jax.ShapeDtypeStruct((DV, DK), BF16),
            jax.ShapeDtypeStruct((1, DK), F32),
        ],
        scratch_shapes=[pltpu.VMEM((DV, DK), F32), pltpu.VMEM((8, DK), F32)],
        cost_estimate=cost(rows * DK * DV * 10, rows * 8192),
        name="blocks",
    )(qkv, qkv, qkv, log_decay)


def parted(a):
    high = a.astype(BF16)
    return high, (a - high.astype(F32)).astype(BF16)


def product(a, b, dims):
    dot = lambda x, y: lax.dot_general(x, y, (dims, ((), ())), preferred_element_type=F32)
    a_parts = (a,) if a.dtype == BF16 else parted(a)
    b_parts = (b,) if b.dtype == BF16 else parted(b)
    total = dot(a_parts[0], b_parts[0])
    if len(a_parts) > 1:
        total = total + dot(a_parts[1], b_parts[0])
    if len(b_parts) > 1:
        total = total + dot(a_parts[0], b_parts[1])
    return total


MESH = pl.DeviceIdType.MESH
A_B, B_A_T, A_T_B = ((1,), (0,)), ((1,), (1,)), ((0,), (0,))


def main_kernel(
    x_ref, gain_ref, low_ref, high_ref, bias_ref, shift_ref, own_a, own_b, own_c,
    init_ref, head_ref, taps_ref,
    attn_ref, filtered_ref, weight_c,
    inner_ref, reach_ref, far_state, glu_ref, far_rim, padded,
    normed, decays, qkv, weight_a, weight_b, state, start, packed,
    z_send, z_recv, f_send, f_recv, s_send, s_recv, r_send, r_recv, *, parts,
):
    place, column = lax.axis_index("sp"), lax.axis_index("fs")
    position = lax.axis_index("tp")
    barrier = pltpu.get_barrier_semaphore()
    partners = [{"sp": lax.rem(place + s, parts)} for s in range(1, parts)]
    partners += [{"fs": column ^ 1}, {"fs": column ^ 2}]
    for partner in partners:
        pl.semaphore_signal(barrier, inc=1, device_id=partner, device_id_type=MESH)
    pl.semaphore_wait(barrier, len(partners))

    owns = (own_a, own_b, own_c)
    weights = (weight_a, weight_b, weight_c)

    def along_z(g, s):
        rows = owns[g].shape[0] // 4
        source = owns[g].at[pl.ds(pl.multiple_of(column * rows, rows), rows), :]
        target = weights[g].at[place * 4 + column]
        return pltpu.make_async_remote_copy(
            src_ref=source,
            dst_ref=target,
            send_sem=z_send.at[g, s - 1],
            recv_sem=z_recv.at[g, s - 1],
            device_id={"sp": lax.rem(place + s, parts)},
            device_id_type=MESH,
        )

    def along_f(g, s, way, mask, held):
        block = lax.rem(place - s + parts, parts) * 4 + (column ^ held)
        return pltpu.make_async_remote_copy(
            src_ref=weights[g].at[block],
            dst_ref=weights[g].at[block],
            send_sem=f_send.at[g, s - 1, way],
            recv_sem=f_recv.at[g, s - 1, way],
            device_id={"fs": column ^ mask},
            device_id_type=MESH,
        )

    def over_x(g, s):
        return along_f(g, s, 0, 1, 0)

    def over_y(g, s):
        return along_f(g, s, 1, 2, 0)

    def diagonal(g, s):
        return along_f(g, s, 2, 1, 2) if (s + g) % 2 else along_f(g, s, 2, 2, 1)

    def on_z(g):
        for s in range(1, parts):
            along_z(g, s).wait_recv()
            over_x(g, s).start()
            over_y(g, s).start()

    def on_f(g):
        for s in range(1, parts):
            over_x(g, s).wait_recv()
            over_y(g, s).wait_recv()
            diagonal(g, s).start()

    def on_diagonal(g):
        for s in range(1, parts):
            diagonal(g, s).wait_recv()

    def state_to(s):
        return pltpu.make_async_remote_copy(
            src_ref=packed,
            dst_ref=far_state.at[s - 1],
            send_sem=s_send.at[s - 1],
            recv_sem=s_recv.at[s - 1],
            device_id={"sp": lax.rem(place + s, parts)},
            device_id_type=MESH,
        )

    def rim_to():
        edge = far_rim.shape[0]
        return pltpu.make_async_remote_copy(
            src_ref=glu_ref.at[glu_ref.shape[0] - edge :, :],
            dst_ref=far_rim,
            send_sem=r_send,
            recv_sem=r_recv,
            device_id={"sp": lax.rem(place + 1, parts)},
            device_id_type=MESH,
        )

    def z_start(g):
        for s in range(1, parts):
            along_z(g, s).start()

    z_start(0)
    for own, weight in zip(owns, weights):
        piece = own.shape[0] // 4
        for i in range(4):
            weight[place * 4 + i] = own[i * piece : (i + 1) * piece, :]

    length = x_ref.shape[0]
    tile = length // 3
    keys = shift_ref.shape[1]
    mine = pl.ds(pl.multiple_of(position * keys, keys), keys)

    def norm_tile(i, none):
        at = pl.ds(pl.multiple_of(i * tile, tile), tile)
        x = x_ref[at, :].astype(F32)
        scale = lax.rsqrt(jnp.mean(x * x, axis=1, keepdims=True) + RMS_EPS)
        rows = (x * scale * gain_ref[...]).astype(BF16)
        normed[at, :] = rows
        low = jnp.dot(rows, low_ref[...], preferred_element_type=F32).astype(BF16)
        z = jnp.dot(low, high_ref[:, mine], preferred_element_type=F32) + bias_ref[:, mine]
        log_sig = jnp.minimum(z, 0.0) - jnp.log1p(jnp.exp(-jnp.abs(z)))
        decays[at, :] = log_sig / GATE_NORMALIZER + shift_ref[at, :]
        return none

    lax.fori_loop(0, 3, norm_tile, 0)
    on_z(0)
    z_start(1)
    on_f(0)
    on_z(1)
    z_start(2)
    on_diagonal(0)

    def times(i, weight):
        at = pl.ds(pl.multiple_of(i * tile, tile), tile)
        full = weight[...].reshape(normed.shape[1], weight.shape[2])
        return at, jnp.dot(normed[at, :], full, preferred_element_type=F32)

    def qkv_tile(i, none):
        at, result = times(i, weight_a)
        qkv[at, :] = result.astype(BF16)
        return none

    lax.fori_loop(0, 3, qkv_tile, 0)

    state[...] = jnp.zeros_like(state)
    start[...] = jnp.zeros_like(start)
    row = lax.broadcasted_iota(jnp.int32, (BLOCK, BLOCK), 0)
    col = lax.broadcasted_iota(jnp.int32, (BLOCK, BLOCK), 1)

    def block_step(i, none):
        at = pl.ds(pl.multiple_of(i * BLOCK, BLOCK), BLOCK)
        lower = (row >= col).astype(BF16)
        decay = decays[at, :]
        high = decay.astype(BF16)
        rest = decay - high.astype(F32)
        middle = rest.astype(BF16)
        least = (rest - middle.astype(F32)).astype(BF16)
        running = (
            jnp.dot(lower, high, preferred_element_type=F32)
            + jnp.dot(lower, middle, preferred_element_type=F32)
            + jnp.dot(lower, least, preferred_element_type=F32)
        )
        final = running[BLOCK - 1 : BLOCK, :]
        before = start[0:1, :]
        q = qkv[at, 0:DK].astype(F32) * DK ** (-0.5)
        k = qkv[at, DK : 2 * DK].astype(F32)
        v = qkv[at, 2 * DK :]
        scaled = q * jnp.exp(running)
        reach_ref[at, :] = scaled * jnp.exp(before)
        scores = product(scaled, k * jnp.exp(-running), B_A_T)
        scores = jnp.where(row >= col, scores, 0.0)
        now = state[...]
        inner_ref[at, :] = product(scores, v, A_B) + product(scaled, now, B_A_T)
        update = product(v, k * jnp.exp(final - running), A_T_B)
        state[...] = jnp.exp(final) * now + update
        start[0:1, :] = before + final
        return none

    count = length // BLOCK
    lax.fori_loop(0, count // 2, block_step, 0)
    on_f(1)
    lax.fori_loop(count // 2, count, block_step, 0)
    total = jnp.exp(start[0:1, :])
    high, low = parted(total)
    width = packed.shape[1]
    packed[:DV, :] = state[...].astype(BF16)
    packed[DV:, :] = jnp.concatenate(
        [
            jnp.broadcast_to(high.astype(F32), (8, width)),
            jnp.broadcast_to(low.astype(F32), (8, width)),
        ],
        axis=0,
    ).astype(BF16)
    on_z(2)
    on_diagonal(1)
    for s in range(1, parts):
        state_to(s).start()

    def glu_tile(i, none):
        at, result = times(i, weight_b)
        half = result.shape[1] // 2
        glu_ref[at, :] = (result[:, :half] * jax.nn.sigmoid(result[:, half:])).astype(BF16)
        return none

    lax.fori_loop(0, 3, glu_tile, 0)
    rim_to().start()
    on_f(2)
    for s in range(1, parts):
        state_to(s).wait()
    carried = jnp.zeros((DV, DK), F32)
    decay = jnp.ones((1, DK), F32)
    for s in range(1, parts):
        other = far_state[s - 1].astype(F32)
        gone = other[DV : DV + 1] + other[DV + 8 : DV + 9]
        carried = carried + jnp.where(place >= s, decay * other[:DV], 0.0)
        decay = decay * jnp.where(place >= s, gone, 1.0)
    state[...] = carried
    start[0:1, :] = decay

    def finish_tile(i, none):
        at = pl.ds(pl.multiple_of(i * tile, tile), tile)
        reach = reach_ref[at, :]
        attended = (
            inner_ref[at, :]
            + product(reach, state[...], B_A_T)
            + product(reach * start[0:1, :], init_ref[...], A_B)
        )
        mean_square = jnp.mean(attended * attended, axis=1, keepdims=True)
        attn_ref[at, :] = (attended * lax.rsqrt(mean_square + RMS_EPS) * head_ref[...]).astype(BF16)
        return none

    lax.fori_loop(0, 3, finish_tile, 0)
    rim_to().wait()
    edge = far_rim.shape[0]
    padded[:edge, :] = jnp.where(place >= 1, far_rim[...].astype(F32), 0.0)
    channels = glu_ref.shape[1]
    ours = pl.ds(pl.multiple_of(position * channels, channels), channels)

    def pad_tile(i, none):
        at = pl.multiple_of(i * tile, tile)
        padded[pl.ds(pl.multiple_of(at + edge, edge), tile), :] = glu_ref[pl.ds(at, tile), :].astype(F32)
        return none

    lax.fori_loop(0, 3, pad_tile, 0)
    rows = 32

    def conv_tile(i, none):
        at = pl.multiple_of(i * rows, rows)
        window = padded[pl.ds(at, rows + edge), :]
        total = jnp.zeros((rows, channels), F32)
        for turn in range(8):
            moved = window if turn == 0 else pltpu.roll(window, rows + edge - turn, 0)
            for j in range(KW):
                offset = j + edge - (KW - 1)
                if offset % 8 == turn:
                    total = total + taps_ref[j : j + 1, ours] * moved[offset - turn : offset - turn + rows]
        filtered_ref[pl.ds(at, rows), :] = total
        return none

    lax.fori_loop(0, length // rows, conv_tile, 0)
    on_diagonal(2)
    for s in range(1, parts):
        for g in range(3):
            along_z(g, s).wait_send()
            over_x(g, s).wait_send()
            over_y(g, s).wait_send()
            diagonal(g, s).wait_send()


def main_call(tokens, gain, low, high, bias, shift, own_a, own_b, own_c, init, head, taps):
    parts = lax.axis_size("sp")
    rows, width = tokens.shape
    piece = own_a.shape[0] // 4
    vmem = pl.BlockSpec(memory_space=pltpu.VMEM)
    shape = jax.ShapeDtypeStruct
    return pl.pallas_call(
        functools.partial(main_kernel, parts=parts),
        in_specs=[vmem] * 12,
        out_specs=[vmem] * 3,
        out_shape=[
            shape((rows, DV), BF16),
            shape((rows, own_b.shape[1] // 2), F32),
            shape((parts * 4, own_c.shape[0] // 4, own_c.shape[1]), BF16),
        ],
        scratch_shapes=[
            pltpu.VMEM((rows, DV), F32),
            pltpu.VMEM((rows, DK), F32),
            pltpu.VMEM((parts - 1, DV + 16, DK), BF16),
            pltpu.VMEM((rows, own_b.shape[1] // 2), BF16),
            pltpu.VMEM((32, own_b.shape[1] // 2), BF16),
            pltpu.VMEM((rows + 32, own_b.shape[1] // 2), F32),
            pltpu.VMEM((rows, width), BF16),
            pltpu.VMEM((rows, DK), F32),
            pltpu.VMEM((rows, own_a.shape[1]), BF16),
            pltpu.VMEM((parts * 4, piece, own_a.shape[1]), BF16),
            pltpu.VMEM((parts * 4, piece, own_b.shape[1]), BF16),
            pltpu.VMEM((DV, DK), F32),
            pltpu.VMEM((8, DK), F32),
            pltpu.VMEM((DV + 16, DK), BF16),
            pltpu.SemaphoreType.DMA((3, parts - 1)),
            pltpu.SemaphoreType.DMA((3, parts - 1)),
            pltpu.SemaphoreType.DMA((3, parts - 1, 3)),
            pltpu.SemaphoreType.DMA((3, parts - 1, 3)),
            pltpu.SemaphoreType.DMA((parts - 1,)),
            pltpu.SemaphoreType.DMA((parts - 1,)),
            pltpu.SemaphoreType.DMA,
            pltpu.SemaphoreType.DMA,
        ],
        compiler_params=pltpu.CompilerParams(
            collective_id=0, has_side_effects=True, vmem_limit_bytes=56 * 2**20
        ),
        cost_estimate=cost(40 * 10**9, 20 * 2**20),
        name="main",
    )(tokens, gain[None], low, high, bias[None], shift, own_a, own_b, own_c, init, head[None], taps)


def finish_kernel(inner_ref, reach_ref, state_ref, gain_ref, out_ref):
    attended = inner_ref[...] + product(reach_ref[...], state_ref[...], B_A_T)
    mean_square = jnp.mean(attended * attended, axis=1, keepdims=True)
    out_ref[...] = (attended * lax.rsqrt(mean_square + RMS_EPS) * gain_ref[...]).astype(BF16)


def finish(inner, reach, state, gain):
    rows = inner.shape[0]
    tile = rows // 3
    tiled = lambda cols: pl.BlockSpec((tile, cols), lambda i: (i, 0))
    return pl.pallas_call(
        finish_kernel,
        grid=(rows // tile,),
        in_specs=[
            tiled(DV),
            tiled(DK),
            pl.BlockSpec((DV, DK), lambda i: (0, 0)),
            pl.BlockSpec((1, DV), lambda i: (0, 0)),
        ],
        out_specs=tiled(DV),
        out_shape=jax.ShapeDtypeStruct((rows, DV), BF16),
        cost_estimate=cost(rows * DK * DV * 2, rows * 4096),
        name="finish",
    )(inner, reach, state, gain[None])


def out_kernel(where, a_ref, c_ref, weight_ref, out_ref):
    half = weight_ref.shape[1] // 2
    out_ref[...] = (
        jnp.dot(a_ref[...], weight_ref[0, :half, :], preferred_element_type=F32)
        + jnp.dot(c_ref[...], weight_ref[0, half:, :], preferred_element_type=F32)
    ).astype(out_ref.dtype)


def out_rows(where, attn, conv, weight, dtype):
    rows, depth = attn.shape
    parts, both, cols = weight.shape
    half = rows // 2
    rowed = pl.BlockSpec((half, depth), lambda z, w: (w[0], 0))
    return pl.pallas_call(
        out_kernel,
        grid_spec=pltpu.PrefetchScalarGridSpec(
            num_scalar_prefetch=1,
            grid=(parts,),
            in_specs=[rowed, rowed, pl.BlockSpec((1, both, cols), lambda z, w: (z, 0, 0))],
            out_specs=pl.BlockSpec((half, cols), lambda z, w: (0, z)),
        ),
        out_shape=jax.ShapeDtypeStruct((half, parts * cols), dtype),
        cost_estimate=cost(2 * half * both * cols * parts, 4 * both * cols * parts),
        name="out_rows",
    )(where, attn, conv, weight)


def on_device(
    tokens,
    norm_gain,
    w_query,
    w_key,
    w_value,
    w_conv_value,
    w_conv_gate,
    w_decay_low,
    w_decay_high,
    gate_bias,
    decay_shift,
    head_gain,
    conv_taps,
    channel_gain,
    w_out_attn,
    w_out_conv,
    init_state,
):
    parts, turns = lax.axis_size("sp"), lax.axis_size("fs")
    place, position = lax.axis_index("sp"), lax.axis_index("tp")
    direct = parts == 4 and turns == 4
    length_here = tokens.shape[1]
    key_cols = w_query.shape[1]
    conv_cols = w_conv_value.shape[1]
    own_qkv = jnp.concatenate([w_query, w_key, w_value], axis=1)
    own_conv = jnp.concatenate([w_conv_value, w_conv_gate], axis=1)
    own_out = jnp.concatenate([w_out_attn, w_out_conv], axis=0)
    if direct:
        attn_out, filtered, out_weight = main_call(
            tokens[0],
            norm_gain,
            w_decay_low,
            w_decay_high,
            gate_bias,
            decay_shift[0],
            own_qkv,
            own_conv,
            own_out,
            init_state[0, 0],
            head_gain,
            conv_taps,
        )
        out_weight = out_weight.reshape(parts, -1, out_weight.shape[2])
    else:
        high_cols = lax.dynamic_slice_in_dim(w_decay_high, position * key_cols, key_cols, 1)
        bias_here = lax.dynamic_slice_in_dim(gate_bias, position * key_cols, key_cols, 0)
        normed, log_decay = norm_and_decay(
            tokens[0], norm_gain, w_decay_low, high_cols, bias_here, decay_shift[0]
        )
        qkv = project(normed, [gathered(own_qkv)], False)
        inner, reach, state, total = blocks(qkv, log_decay)
        high, low = parted(total)
        edges = [jnp.broadcast_to(part, (8, DK)) for part in (high, low)]
        packed = jnp.concatenate([state, *edges], axis=0)
        others = [shifted(packed, "sp", s) for s in range(1, parts)]
        glu = project(normed, [gathered(own_conv)], True)
        rim = shifted(glu[length_here - 32 :], "sp", 1)
        out_weight = lax.all_gather(own_out, "sp", axis=1, tiled=True)
        carried = jnp.zeros((DV, DK), F32)
        decay = jnp.ones((1, DK), F32)
        for s in range(1, parts):
            other = others[s - 1].astype(F32)
            gone = other[DV : DV + 1] + other[DV + 8 : DV + 9]
            carried = carried + jnp.where(place >= s, decay * other[:DV], 0.0)
            decay = decay * jnp.where(place >= s, gone, 1.0)
        incoming = carried + decay * init_state[0, 0].T
        attn_out = finish(inner, reach, incoming, head_gain)

        rim = jnp.where(place >= 1, rim[rim.shape[0] - (KW - 1) :], jnp.zeros((), BF16))
        padded = jnp.concatenate([rim, glu], axis=0).astype(F32)
        taps_here = lax.dynamic_slice_in_dim(conv_taps, position * conv_cols, conv_cols, 1)
        filtered = jnp.zeros((length_here, conv_cols), F32)
        for tap_index in range(KW):
            filtered = filtered + taps_here[tap_index] * padded[tap_index : tap_index + length_here]
    first_sum, square_sum = lax.psum(
        (
            jnp.sum(filtered, axis=1, keepdims=True),
            jnp.sum(filtered * filtered, axis=1, keepdims=True),
        ),
        "tp",
    )
    mean = first_sum / CW
    centered = filtered - mean
    variance = square_sum / CW - mean * mean
    gain_here = lax.dynamic_slice_in_dim(channel_gain, position * conv_cols, conv_cols, 0)
    conv_out = jax.nn.silu(centered * lax.rsqrt(variance + LN_EPS) * gain_here).astype(BF16)

    if direct:
        at = lambda half: half.astype(jnp.int32)[None]
        given = out_rows(at(1 - position), attn_out, conv_out, out_weight, BF16)
        taken = lax.ppermute(given, "tp", [(0, 1), (1, 0)])
        kept = out_rows(at(position), attn_out, conv_out, out_weight, F32)
    else:
        both = jnp.concatenate([attn_out, conv_out], axis=1)
        columns = jnp.dot(both, out_weight, preferred_element_type=F32)
        half = length_here // 2
        kept = lax.dynamic_slice_in_dim(columns, position * half, half, 0)
        given = lax.dynamic_slice_in_dim(columns, (1 - position) * half, half, 0).astype(BF16)
        taken = lax.ppermute(given, "tp", [(0, 1), (1, 0)])
    return (kept + taken.astype(F32)).astype(BF16)[None]


def solution(mesh):
    in_specs = (
        P("fs", "sp", None),
        P(),
        P("sp", "tp"),
        P("sp", "tp"),
        P("sp", "tp"),
        P("sp", "tp"),
        P("sp", "tp"),
        P(),
        P(),
        P(),
        P("fs", "sp", "tp"),
        P(),
        P(),
        P(),
        P("tp", "sp"),
        P("tp", "sp"),
        P("fs", "tp", None, None),
    )
    out_specs = P("fs", ("sp", "tp"), None)
    return jax.shard_map(
        on_device, mesh=mesh, in_specs=in_specs, out_specs=out_specs, check_vma=False
    )
```
